32 devices in a mesh: sp: 8 (over z, y), tp: 4 (over x, core).
Axes of the slice: x: 2, y: 2, z: 4, core: 2. Of those that a mesh axis runs over, the one named last changes fastest.
Arguments:
- stream: bfloat16 [1024, 2048], P('sp', 'tp'), may hold values from -40 to 40
- queries: bfloat16 [1024, 1024], P('sp', 'tp'), may hold values from -6 to 6
- keys: bfloat16 [1024, 1024], P('sp', 'tp'), may hold values from -6 to 6
- values: bfloat16 [1024, 2048], P('sp', 'tp'), may hold values from -25 to 25
- out_gate: bfloat16 [1024, 2048], P('sp', 'tp'), may hold values from -8 to 8
- input_gate: float32 [1024, 8], P('sp', 'tp'), may hold values from -9 to 350
- forget_gate: float32 [1024, 8], P('sp', 'tp'), may hold values from -4 to 20
- head_gain: float32 [2048], P('tp'), may hold values from 0.1 to 1.9
- w_out: bfloat16 [2048, 2048], P('tp'), may hold values from -0.125 to 0.125
- ffn_gain: float32 [2048], replicated, may hold values from 0.1 to 1.9
- w_gate: bfloat16 [2048, 5632], P('sp', 'tp'), may hold values from -0.125 to 0.125
- w_up: bfloat16 [2048, 5632], P('sp', 'tp'), may hold values from -0.125 to 0.125
- w_down: bfloat16 [5632, 2048], P('tp', 'sp'), may hold values from -0.078125 to 0.078125
Outputs:
- mixed: bfloat16 [1024, 2048], P('sp', 'tp')
The draws below stay inside these ranges and needn't reach their ends.
All inputs are finite; a program needn't handle non-finite values.
Results may differ from the reference program's by a relative error of at most 0.0095.
Values may be sent and summed in bfloat16 or wider, within the bound.
A program may use at most 128 MiB of HBM per device.

```python
import math
import jax
import jax.numpy as jnp
from jax import lax

D = 2048
HEADS = 8
DQK = 128
DV = 256
FF = 5632
BLOCK = 64
TOK_DEV = 128
SEQUENCE_TOKENS = 1024
VALS = 2048
N_SP = 8
N_TP = 4


def draw_stream(key, part):
    first, second = jax.random.split(jax.random.fold_in(key, 11), 2)
    rising = 3.0 ** (jnp.arange(D, dtype=jnp.float32) / D)
    rough = jnp.exp(jax.random.uniform(second, (D,), jnp.float32, -0.5, 0.5))
    full = jnp.clip(jax.random.normal(first, (SEQUENCE_TOKENS, D), jnp.float32), -5.0, 5.0) * rising * rough
    return full.astype(jnp.bfloat16)


def draw_values(key, part):
    first, second = jax.random.split(jax.random.fold_in(key, 41), 2)
    head_place = (jnp.arange(VALS) // DV).astype(jnp.float32)
    rising = 3.0 ** (head_place / (HEADS - 1))
    rough = jnp.exp(jax.random.uniform(second, (VALS,), jnp.float32, -0.5, 0.5))
    base = jnp.clip(jax.random.normal(first, (SEQUENCE_TOKENS, VALS), jnp.float32), -5.0, 5.0)
    return (base * rising * rough).astype(jnp.bfloat16)


def draw_input_gate(key, part):
    first = jax.random.fold_in(jax.random.fold_in(key, 23), 0)
    base = jnp.clip(1.5 * jax.random.normal(first, (SEQUENCE_TOKENS, HEADS), jnp.float32), -9.0, 9.0)
    return base


def draw_forget_gate(key, part):
    partition_key = jax.random.split(jax.random.fold_in(key, 37), 6)
    fast_share = 0.5
    fast = jax.random.uniform(partition_key[0], (HEADS,), jnp.float32) < fast_share
    fast_rate = 1.0 / jax.random.uniform(partition_key[1], (HEADS,), jnp.float32, 30.0, 100.0)
    slow_rate = 0.12 * math.log(10.0) / SEQUENCE_TOKENS
    factor = jnp.exp(jax.random.uniform(partition_key[2], (SEQUENCE_TOKENS // TOK_DEV, 1), jnp.float32, -math.log(2.0), math.log(2.0)))
    factor = jnp.repeat(factor, TOK_DEV, axis=0)
    speed_ratio = jnp.where(fast, fast_rate, slow_rate)[None, :] * factor
    position_slots = jax.random.randint(partition_key[3], (3,), 0, SEQUENCE_TOKENS)
    spike_events = jnp.any(jnp.arange(SEQUENCE_TOKENS)[:, None] == position_slots[None, :], axis=1)[:, None]
    spike_frequency = -jnp.log(jax.random.uniform(partition_key[4], (SEQUENCE_TOKENS, 1), jnp.float32, 0.55, 0.8))
    speed_ratio = jnp.where(spike_events, spike_frequency, speed_ratio)
    noise = jnp.clip(0.7 * jax.random.normal(partition_key[5], (SEQUENCE_TOKENS, HEADS), jnp.float32), -2.0, 2.0)
    return -jnp.log(jnp.expm1(speed_ratio)) + noise


def block_levels(key, dims, cuts, least, top_value):
    loudness, own = 1.0, jax.random.fold_in(key, 6)
    for axis_at, blocks in cuts:
        heights = jnp.exp(jax.random.uniform(jax.random.fold_in(own, axis_at), (blocks,), jnp.float32, least / len(cuts), top_value / len(cuts)))
        loudness = loudness * jnp.repeat(heights, dims[axis_at] // blocks).reshape([-1 if axis == axis_at else 1 for axis in range(len(dims))])
    return loudness


def normal_values(rng, dims, scale, reach, shards=(), kind=jnp.bfloat16):
    drawn = scale * jax.random.normal(rng, dims, jnp.float32)
    if shards:
        drawn = drawn * block_levels(rng, dims, shards, -0.22, 0.18)
    return jnp.clip(drawn, -reach, reach).astype(kind)


def setup_inputs(seed: int = 0) -> dict:
    seeds = jax.random.split(jax.random.key(seed), 14)
    return {
        "stream": draw_stream(jax.random.fold_in(seeds[13], 71), 0),
        "queries": normal_values(seeds[1], (SEQUENCE_TOKENS, HEADS * DQK), 1.0, 6.0, ((0, 8), (1, 4))),
        "keys": normal_values(seeds[2], (SEQUENCE_TOKENS, HEADS * DQK), 1.0, 6.0, ((0, 8), (1, 4))),
        "values": draw_values(jax.random.fold_in(seeds[13], 71), 0),
        "out_gate": normal_values(seeds[4], (SEQUENCE_TOKENS, VALS), 1.5, 8.0, ((0, 8), (1, 4))),
        "input_gate": draw_input_gate(jax.random.fold_in(seeds[13], 71), 0),
        "forget_gate": draw_forget_gate(jax.random.fold_in(seeds[13], 71), 0),
        "head_gain": jnp.clip(1.0 + 0.18 * jax.random.normal(seeds[7], (VALS,), jnp.float32), 0.1, 1.9),
        "w_out": normal_values(seeds[8], (VALS, D), VALS ** -0.5, 0.125, ((0, 4),)),
        "ffn_gain": jnp.clip(1.0 + 0.18 * jax.random.normal(seeds[9], (D,), jnp.float32), 0.1, 1.9),
        "w_gate": normal_values(seeds[10], (D, FF), D ** -0.5, 0.125, ((0, 8), (1, 4))),
        "w_up": normal_values(seeds[11], (D, FF), D ** -0.5, 0.125, ((0, 8), (1, 4))),
        "w_down": normal_values(seeds[12], (FF, D), FF ** -0.5, 0.078125, ((0, 4), (1, 8))),
    }


precise = lax.Precision.HIGHEST
norm_eps = 1e-06
very_low = -1e+30

def block_summary(key_blk, value_blk, input_blk, decay_sum):
    decay_total = decay_sum[..., -1]
    log_weight = decay_total[..., None] - decay_sum + input_blk
    weight_peak = lax.optimization_barrier(jnp.max(log_weight, axis=-1))
    weights = jnp.exp(log_weight - weight_peak[..., None])
    state_mat = jnp.einsum('...ld,...le->...de', weights[..., None] * key_blk, value_blk, precision=precise)
    state_vec = jnp.einsum('...l,...ld->...d', weights, key_blk, precision=precise)
    return (state_mat, state_vec, weight_peak, decay_total)

def combine(earlier, later):
    ceiling = jnp.maximum(later[3] + earlier[2], later[2])
    former = jnp.exp(later[3] + earlier[2] - ceiling)
    latter = jnp.exp(later[2] - ceiling)
    return (former[..., None, None] * earlier[0] + latter[..., None, None] * later[0], former[..., None] * earlier[1] + latter[..., None] * later[1], ceiling, earlier[3] + later[3])

def block_output(query_blk, key_blk, value_blk, input_blk, decay_sum, state_mat, state_vec, state_peak):
    block_len = query_blk.shape[-2]
    causal = jnp.tril(jnp.ones((block_len, block_len), jnp.bool_))
    log_pair = jnp.where(causal, decay_sum[..., :, None] - decay_sum[..., None, :] + input_blk[..., None, :], -jnp.inf)
    log_carry = decay_sum + state_peak[..., None]
    row_peak = jnp.maximum(log_carry, lax.optimization_barrier(jnp.max(log_pair, axis=-1)))
    scores = jnp.einsum('...ld,...sd->...ls', query_blk, key_blk, precision=precise) * jnp.exp(log_pair - row_peak[..., None])
    carried = jnp.exp(log_carry - row_peak)
    numer = jnp.einsum('...ls,...se->...le', scores, value_blk, precision=precise) + carried[..., None] * jnp.einsum('...ld,...de->...le', query_blk, state_mat, precision=precise)
    normer = lax.optimization_barrier(jnp.sum(scores, axis=-1)) + carried * jnp.einsum('...ld,...d->...l', query_blk, state_vec, precision=precise)
    denom = jnp.maximum(jnp.abs(normer), jnp.exp(-row_peak))
    return numer / denom[..., None]

def reference(stream, queries, keys, values, out_gate, input_gate, forget_gate, head_gain, w_out, ffn_gain, w_gate, w_up, w_down):
    blocks = SEQUENCE_TOKENS // BLOCK

    def to_blocks(array, col_width):
        return array.reshape(blocks, BLOCK, HEADS, col_width).transpose(0, 2, 1, 3)
    query_all = to_blocks(queries, DQK)
    key_all = to_blocks(keys, DQK)
    value_all = to_blocks(values, DV)
    input_all = input_gate.reshape(blocks, BLOCK, HEADS).transpose(0, 2, 1)
    forget_all = forget_gate.reshape(blocks, BLOCK, HEADS).transpose(0, 2, 1)

    def advance(carry, pieces):
        query_blk = pieces[0].astype(jnp.float32) * DQK ** (-0.5)
        key_blk = pieces[1].astype(jnp.float32)
        value_blk = pieces[2].astype(jnp.float32)
        decay_sum = jnp.cumsum(jax.nn.log_sigmoid(pieces[4]), axis=-1)
        output = block_output(query_blk, key_blk, value_blk, pieces[3], decay_sum, carry[0], carry[1], carry[2])
        return (combine(carry, block_summary(key_blk, value_blk, pieces[3], decay_sum)), output)
    start = (jnp.zeros((HEADS, DQK, DV), jnp.float32), jnp.zeros((HEADS, DQK), jnp.float32), jnp.full((HEADS,), very_low, jnp.float32), jnp.zeros((HEADS,), jnp.float32))
    _, mixed_heads = lax.scan(advance, start, (query_all, key_all, value_all, input_all, forget_all))
    head_rows = mixed_heads.transpose(0, 2, 1, 3).reshape(SEQUENCE_TOKENS, HEADS, DV)
    mean_sq = lax.optimization_barrier(jnp.mean(head_rows * head_rows, axis=(1, 2), keepdims=True))
    gated = head_rows * lax.rsqrt(mean_sq + norm_eps) * head_gain.reshape(HEADS, DV) * jax.nn.sigmoid(out_gate.astype(jnp.float32).reshape(SEQUENCE_TOKENS, HEADS, DV))
    heads_out = gated.reshape(SEQUENCE_TOKENS, HEADS * DV).astype(jnp.bfloat16)
    group = HEADS * DV // N_TP
    mixer = jnp.zeros((SEQUENCE_TOKENS, D), jnp.float32)
    for member in range(N_TP):
        partial_value = jnp.dot(heads_out[:, member * group:(member + 1) * group], w_out[member * group:(member + 1) * group], preferred_element_type=jnp.float32).astype(jnp.bfloat16)
        mixer = mixer + lax.optimization_barrier(partial_value).astype(jnp.float32)
    resid = (stream.astype(jnp.float32) + mixer).astype(jnp.bfloat16)
    hidden_group = FF // N_TP

    def channel_mix(rows_in):
        rows_float = rows_in.astype(jnp.float32)
        normed = (rows_float * lax.rsqrt(lax.optimization_barrier(jnp.mean(rows_float * rows_float, axis=-1, keepdims=True)) + norm_eps) * ffn_gain).astype(jnp.bfloat16)
        gate_act = jnp.dot(normed, w_gate, preferred_element_type=jnp.float32)
        up_act = jnp.dot(normed, w_up, preferred_element_type=jnp.float32)
        hidden = (jax.nn.silu(gate_act) * up_act).astype(jnp.bfloat16)
        totals = jnp.zeros((rows_in.shape[0], D), jnp.float32)
        for member in range(N_TP):
            partial_value = jnp.dot(hidden[:, member * hidden_group:(member + 1) * hidden_group], w_down[member * hidden_group:(member + 1) * hidden_group], preferred_element_type=jnp.float32).astype(jnp.bfloat16)
            totals = totals + lax.optimization_barrier(partial_value).astype(jnp.float32)
        return (rows_float + totals).astype(jnp.bfloat16)
    mixed = lax.map(channel_mix, resid.reshape(N_SP, TOK_DEV, D))
    return mixed.reshape(SEQUENCE_TOKENS, D)
```

```python
import functools

import jax
import jax.numpy as jnp
from jax import lax
from jax.experimental import pallas as pl
from jax.experimental.pallas import tpu as pltpu
from jax.sharding import PartitionSpec as P

D = 2048
DQK = 128
DV = 256
BLOCK = 64
VALS = 2048


precise = lax.Precision.HIGHEST
norm_eps = 1e-06
very_low = -1e30


def entering(value, axis, join, neutral):
    count, mine = (lax.axis_size(axis), lax.axis_index(axis))
    pieces = jax.tree.map(lambda part: lax.all_gather(part, axis), value)
    subtotal = jax.tree.map(
        lambda part, zero: jnp.full_like(part, 0) + jnp.asarray(zero, part.dtype), value, neutral
    )

    def step(position, subtotal):
        longer = join(subtotal, jax.tree.map(lambda part: part[position], pieces))
        return jax.tree.map(lambda new, old: jnp.where(position < mine, new, old), longer, subtotal)

    return lax.fori_loop(0, count - 1, step, subtotal)


def block_summary(key_blk, value_blk, input_blk, decay_sum):
    decay_total = decay_sum[..., -1]
    log_weight = decay_total[..., None] - decay_sum + input_blk
    weight_peak = jnp.max(log_weight, axis=-1)
    weights = jnp.exp(log_weight - weight_peak[..., None])
    state_mat = jnp.einsum(
        "...ld,...le->...de", weights[..., None] * key_blk, value_blk, precision=precise
    )
    state_vec = jnp.einsum("...l,...ld->...d", weights, key_blk, precision=precise)
    return (state_mat, state_vec, weight_peak, decay_total)


def combine(earlier, later):
    ceiling = jnp.maximum(later[3] + earlier[2], later[2])
    former = jnp.exp(later[3] + earlier[2] - ceiling)
    latter = jnp.exp(later[2] - ceiling)
    return (
        former[..., None, None] * earlier[0] + latter[..., None, None] * later[0],
        former[..., None] * earlier[1] + latter[..., None] * later[1],
        ceiling,
        earlier[3] + later[3],
    )


def block_output(
    query_blk, key_blk, value_blk, input_blk, decay_sum, state_mat, state_vec, state_peak
):
    block_len = query_blk.shape[-2]
    causal = jnp.tril(jnp.ones((block_len, block_len), jnp.bool_))
    log_pair = jnp.where(
        causal,
        decay_sum[..., :, None] - decay_sum[..., None, :] + input_blk[..., None, :],
        -jnp.inf,
    )
    log_carry = decay_sum + state_peak[..., None]
    row_peak = jnp.maximum(log_carry, jnp.max(log_pair, axis=-1))
    scores = jnp.einsum("...ld,...sd->...ls", query_blk, key_blk, precision=precise) * jnp.exp(
        log_pair - row_peak[..., None]
    )
    carried = jnp.exp(log_carry - row_peak)
    numer = jnp.einsum("...ls,...se->...le", scores, value_blk, precision=precise) + carried[
        ..., None
    ] * jnp.einsum("...ld,...de->...le", query_blk, state_mat, precision=precise)
    normer = jnp.sum(scores, axis=-1) + carried * jnp.einsum(
        "...ld,...d->...l", query_blk, state_vec, precision=precise
    )
    denom = jnp.maximum(jnp.abs(normer), jnp.exp(-row_peak))
    return numer / denom[..., None]


def local(
    stream,
    queries,
    keys,
    values,
    out_gate,
    input_gate,
    forget_gate,
    head_gain,
    w_out,
    ffn_gain,
    w_gate,
    w_up,
    w_down,
):
    gate_full, up_full, down_full = (
        lax.all_gather(w_gate, "sp", axis=0, tiled=True),
        lax.all_gather(w_up, "sp", axis=0, tiled=True),
        lax.all_gather(w_down, "sp", axis=1, tiled=True),
    )
    count_of_rows = stream.shape[0]
    head_count = input_gate.shape[1]
    blocks = count_of_rows // BLOCK

    def to_blocks(array, col_width):
        return (
            array.astype(jnp.float32)
            .reshape(blocks, BLOCK, head_count, col_width)
            .transpose(2, 0, 1, 3)
        )

    query_blk = to_blocks(queries, DQK) * DQK ** (-0.5)
    key_blk = to_blocks(keys, DQK)
    value_blk = to_blocks(values, DV)
    input_blk = input_gate.reshape(blocks, BLOCK, head_count).transpose(2, 0, 1)
    decay_sum = jnp.cumsum(
        jax.nn.log_sigmoid(forget_gate).reshape(blocks, BLOCK, head_count).transpose(2, 0, 1),
        axis=-1,
    )
    summary = block_summary(key_blk, value_blk, input_blk, decay_sum)
    identity = (
        jnp.zeros((head_count, DQK, DV), jnp.float32),
        jnp.zeros((head_count, DQK), jnp.float32),
        jnp.full((head_count,), very_low, jnp.float32),
        jnp.zeros((head_count,), jnp.float32),
    )

    def advance(carry, piece):
        return (combine(carry, piece), carry)

    local_total, prefix = lax.scan(
        advance, identity, jax.tree.map(lambda array: jnp.moveaxis(array, 1, 0), summary)
    )
    carry_in = entering(local_total, "sp", combine, identity)
    start = combine(
        jax.tree.map(lambda array: array[:, None], carry_in),
        jax.tree.map(lambda array: jnp.moveaxis(array, 0, 1), prefix),
    )
    mixed_heads = block_output(
        query_blk, key_blk, value_blk, input_blk, decay_sum, start[0], start[1], start[2]
    )
    head_rows = mixed_heads.transpose(1, 2, 0, 3).reshape(count_of_rows, head_count, DV)
    local_sq = jnp.sum(head_rows * head_rows, axis=(1, 2))
    total_sq = lax.psum(local_sq, "tp")
    row_scale = lax.rsqrt(total_sq / VALS + norm_eps)
    gated = (
        head_rows
        * row_scale[:, None, None]
        * head_gain.reshape(head_count, DV)
        * jax.nn.sigmoid(out_gate.astype(jnp.float32).reshape(count_of_rows, head_count, DV))
    )
    heads_out = gated.reshape(count_of_rows, head_count * DV).astype(jnp.bfloat16)
    partial_value = jnp.dot(heads_out, w_out, preferred_element_type=jnp.float32)
    col_width = stream.shape[1]
    col_start = lax.axis_index("tp") * col_width
    mixer_own = lax.psum_scatter(
        partial_value.astype(jnp.bfloat16), "tp", scatter_dimension=1, tiled=True
    ).astype(jnp.float32)
    resid_own = (stream.astype(jnp.float32) + mixer_own).astype(jnp.bfloat16)
    resid_f = resid_own.astype(jnp.float32)
    square_total = lax.psum(jnp.sum(resid_f * resid_f, axis=-1), "tp")
    gain_own = lax.dynamic_slice_in_dim(ffn_gain, col_start, col_width)
    normed_own = (resid_f * lax.rsqrt(square_total / D + norm_eps)[:, None] * gain_own).astype(
        jnp.bfloat16
    )
    normed = lax.all_gather(normed_own, "tp", axis=1, tiled=True)
    gate_act = jnp.dot(normed, gate_full, preferred_element_type=jnp.float32)
    up_act = jnp.dot(normed, up_full, preferred_element_type=jnp.float32)
    hidden = (jax.nn.silu(gate_act) * up_act).astype(jnp.bfloat16)
    term = jnp.dot(hidden, down_full, preferred_element_type=jnp.float32)
    down_own = lax.psum_scatter(
        term.astype(jnp.bfloat16), "tp", scatter_dimension=1, tiled=True
    ).astype(jnp.float32)
    return (resid_own.astype(jnp.float32) + down_own).astype(jnp.bfloat16)


def remote(src, dst, send, recv, target):
    return pltpu.make_async_remote_copy(
        src_ref=src,
        dst_ref=dst,
        send_sem=send,
        recv_sem=recv,
        device_id=target,
        device_id_type=pl.DeviceIdType.MESH,
    )


COPIES = 256
SUMS = 28


def fused_kernel(
    n, m, heads, stream_h, q_h, k_h, v_h, og_h, f_ref, i_ref, hg_ref, wo_h, fg_ref, wg_h, wu_h, wd_h,
    out_ref, kvb, gb, stb, qb, ogb, wob, wgb, wub, wtb, gub, db, pb, pxb, xb, hb, ob, rb, sqb,
    resb, ssem, rsem, lsem, note,
):
    rows, width = out_ref.shape
    ring = n // 2
    half = rows // 2
    dv = width // heads
    dqk = qb.shape[1] // heads
    part, depth = wtb.shape[2], wtb.shape[3]
    room = gub.shape[3]
    low = jnp.bfloat16
    s, t = lax.axis_index("sp"), lax.axis_index("tp")
    z, y, x, c = s // 2, s % 2, t // 2, t % 2
    lead, middle = z % 2 == c, (z == 1) | (z == 2)
    zs = [2 * ((z // 2 + d // 2) % 2) + (z + d) % 2 for d in range(ring)]
    ys, xs, cs = ([y, 1 - y], [x, 1 - x], [c, 1 - c])
    ranks = [[zs[oz] * 2 + ys[oe] for oe in range(2)] for oz in range(ring)]
    cores = [[xs[ox] * 2 + cs[oc] for oc in range(2)] for ox in range(2)]
    places_x = [[xs[ox] * 2 + ty for ty in range(2)] for ox in range(2)]
    places_z = [v // 2 for v in zs]
    at = lambda oz, oe: ranks[oz][oe]
    to = lambda oz=0, oe=0, ox=0, oc=0: (at(oz, oe), cores[ox][oc])
    under = [[(z + ring - d) % ring * 2 + ys[oe] for oe in range(2)] for d in range(ring)]
    above = ((z + 1) % ring * 2 + y, t)
    home = x == z // 2
    branches = {
        "all": None,
        "lead home": lead & home,
        "lead away": lead & jnp.logical_not(home),
        "lead": lead,
        "other": jnp.logical_not(lead),
        "lead0": lead & (c == 0),
        "lead1": lead & (c == 1),
        "lead mid": lead & middle,
        "other mid": jnp.logical_not(lead) & middle,
        "other end": jnp.logical_not(lead | middle),
        "lead end": lead & jnp.logical_not(middle),
        "low y": y == 0,
        "lower": z < 2,
        "upper": z >= 2,
    }
    for d in range(ring):
        branches["at", d] = z == d
        branches["from", d] = z >= d
        branches["up", d] = (z >= d) & (z < ring - 1)

    def when(branch):
        return pl.when(branches[branch])

    first, second = slice(0, half), slice(half, rows)
    places, begun, spots = {}, {}, {}

    def place(key):
        i = places.setdefault(key, len(places))
        assert i < COPIES
        return i

    def begin(branch, key, src, dst, target, tag=""):
        def make():
            return remote(
                src(), dst(), ssem.at[place((key, tag))], rsem.at[place((key, ""))], target
            )

        make().start()
        begun.setdefault(branch, {})[key, tag] = make

    def arrive(key, ref):
        i = place((key, ""))
        remote(ref, ref, ssem.at[i], rsem.at[i], to(0, 0, 0, 1)).wait_recv()

    def spot(key):
        i = spots.setdefault(key, len(spots))
        assert i < SUMS
        return rb.at[i]

    count = [0]

    def local(src, dst):
        copy = pltpu.make_async_copy(src, dst, lsem.at[count[0]])
        count[0] += 1
        copy.start()
        return copy

    qk = heads * dqk
    load_kv = [local(k_h, kvb.at[s, :, :qk]), local(v_h, kvb.at[s, :, qk:])]
    load_w = [local(wg_h, wgb), local(wu_h, wub)]
    load_g = [local(f_ref, gb.at[s, 0]), local(i_ref, gb.at[s, 1])]
    load_cell = [local(q_h, qb), local(og_h, ogb)]
    load_rest = [local(wo_h, wob), local(stream_h, stb.at[c])]

    barrier = pltpu.get_barrier_semaphore()
    peers = [to(oz, oe) for oz in range(ring) for oe in range(2) if oz or oe]
    peers += [to(0, 0, ox, oc) for ox in range(2) for oc in range(2) if ox or oc]
    peers += [to(2, 0, 0, 1)]
    for peer in peers:
        pl.semaphore_signal(barrier, inc=1, device_id=peer, device_id_type=pl.DeviceIdType.MESH)
    pl.semaphore_wait(barrier, len(peers))

    others = [(oz, oe) for oz in range(ring) for oe in range(2) if oz or oe]
    for oz, oe in others:
        for w, ref in enumerate((f_ref, i_ref)):
            begin(
                "all", ("g", w, oz, oe), lambda ref=ref: ref, lambda w=w: gb.at[s, w],
                to(oz, oe),
            )

    def piece_kv(d, oe, rows_of):
        return kvb.at[under[d][oe]].at[rows_of]

    def kv(branch, d, way, rows_of):
        up = way == "up"
        key = ("kv", d + up, 1 - up, rows_of is second)
        ref = lambda: piece_kv(d, 0, rows_of)
        begin(branch, key, ref, ref, above if up else to(0, 1))

    def kv_in(d, oe, rows_of):
        arrive(("kv", d, oe, rows_of is second), piece_kv(d, oe, rows_of))

    for copy in load_kv:
        copy.wait()

    for rows_of in (first, second):

        @when(("up", 0))
        def _():
            kv(("up", 0), 0, "up", rows_of)

        @when("low y")
        def _():
            kv("low y", 0, "across", rows_of)

    for j in range(1, n - 1):

        @pl.when(j > s)
        def _():
            kvb[j] = jnp.zeros(kvb.shape[1:], low)

    zero = jnp.zeros((room - part, depth), low)
    for k in range(n):
        for core in range(2):
            for w in range(2):
                gub[k, w, core, part:] = zero
                if k < n // 2:
                    db[k, w, core, part:] = zero
    for copy in load_w:
        copy.wait()
    lanes = 128
    for w, source in enumerate((wgb, wub)):
        for q in range(source.shape[1] // lanes):
            turned = source[:, q * lanes : (q + 1) * lanes].T
            cut = q * lanes
            while cut < (q + 1) * lanes:
                stop = min((cut // part + 1) * part, (q + 1) * lanes)
                off = cut % part
                wtb[cut // part, w, off : off + stop - cut] = turned[cut - q * lanes : stop - q * lanes]
                cut = stop

    gu_at = lambda k: gub.at[k, :, c, :part]
    d_at = lambda k: db.at[k, :, c, :part]

    def weights(branch, oz, oe):
        k = at(oz, oe)
        begin(branch, ("gu", oz, oe), lambda: wtb.at[k], lambda: gu_at(s), to(oz, oe))

    quarters = [[zs[oz] % 2 * 2 + ys[oe] for oe in range(2)] for oz in range(2)]
    mine = quarters[0][0]

    def weights_d(oz, oe):
        k = quarters[oz][oe]
        begin("all", ("d", oz, oe), lambda: wd_h.at[:, k], lambda: d_at(mine), to(oz, oe))

    load_own = [local(wtb.at[s], gu_at(s)), local(wd_h.at[:, mine], d_at(mine))]

    near = [(0, 1), (1, 0), (1, 1)]
    far = [(2, 0), (3, 0), (2, 1), (3, 1)]
    plan = {
        0: ([(1, 0), (1, 1), (0, 1)], [], [], far),
        1: ([(1, 0)], [(3, 0), (3, 1), (2, 0), (2, 1)], [], [(0, 1), (1, 1)]),
        2: ([(3, 0), (2, 0)], [], [(1, 0), (3, 1), (1, 1), (2, 1)], [(0, 1)]),
        3: ([(2, 0), (3, 0), (1, 0)], [], [(2, 1), (3, 1)], [(0, 1), (1, 1)]),
    }

    def issue(phase):
        for at_z, phases in plan.items():
            if phases[phase]:

                @when(("at", at_z))
                def _():
                    for oz, oe in phases[phase]:
                        weights(("at", at_z), oz, oe)

    issue(0)

    for d in range(1, ring):
        for rows_of in (first, second):

            @when(("from", d))
            def _():
                kv_in(d, 0, rows_of)
                if d < ring - 1:

                    @when(("up", d))
                    def _():
                        kv(("up", d), d, "up", rows_of)

                kv(("from", d), d, "across", rows_of)

    note_partner = lambda i: pl.semaphore_signal(
        note.at[i], inc=1, device_id=to(0, 0, 0, 1), device_id_type=pl.DeviceIdType.MESH
    )
    note_partner(1)
    pl.semaphore_wait(note.at[1], 1)

    issue(1)

    for rows_of in (first, second):

        @pl.when(y == 1)
        def _():
            kv_in(0, 1, rows_of)

        for d in range(1, ring):

            @when(("from", d))
            def _():
                kv_in(d, 1, rows_of)

    issue(2)
    for oz, oe in others:
        for w in range(2):
            arrive(("g", w, oz, oe), gb.at[at(oz, oe), w])
    for copy in load_cell + load_g + load_rest:
        copy.wait()

    @when("other")
    def _():
        begin("other", ("st",), lambda: stb.at[c], lambda: stb.at[c], to(0, 0, 0, 1))

    at_row = lax.broadcasted_iota(jnp.int32, (rows, rows), 0)
    at_col = lax.broadcasted_iota(jnp.int32, (rows, rows), 1)
    eye, causal = at_row == at_col, at_row >= at_col
    to_column = lambda row: jnp.sum(jnp.where(eye, row, 0.0), axis=1, keepdims=True)
    upper = (at_row <= at_col).astype(jnp.float32)
    gates = jnp.concatenate([gb[j, 0] for j in range(n)], axis=0)
    entries = jnp.concatenate([gb[j, 1] for j in range(n)], axis=0)
    log_sigmoid = lambda v: jnp.minimum(v, 0.0) - jnp.log1p(jnp.exp(-jnp.abs(v)))
    decays = jnp.dot(
        log_sigmoid(gates), upper, precision=precise, preferred_element_type=jnp.float32
    )
    own_decay = jnp.dot(
        log_sigmoid(f_ref[...]), upper, precision=precise, preferred_element_type=jnp.float32
    )
    own_entry = i_ref[...]
    square = jnp.zeros((rows, 1), jnp.float32)
    gated = []
    for h in range(heads):
        decay_row = own_decay[h : h + 1]
        decay_col = to_column(decay_row)
        after = jnp.zeros((1, 1), jnp.float32)
        peak = jnp.full((1, 1), very_low, jnp.float32)
        weigh = [None] * n
        for j in reversed(range(n)):
            earlier = j < s
            block = decays[j * heads + h : j * heads + h + 1]
            total = block[:, rows - 1 :]
            entry = entries[j * heads + h : j * heads + h + 1]
            weigh[j] = jnp.where(earlier, total - block + entry + after, very_low)
            after = after + jnp.where(earlier, total, 0.0)
            peak = jnp.maximum(peak, jnp.max(weigh[j], axis=1, keepdims=True))
        pair = jnp.where(causal, decay_col - decay_row + own_entry[h : h + 1], very_low)
        row_peak = jnp.maximum(decay_col + peak, jnp.max(pair, axis=1, keepdims=True))
        query = qb[:, h * dqk : (h + 1) * dqk]
        numer = jnp.zeros((rows, dv), jnp.float32)
        normer = jnp.zeros((rows, 1), jnp.float32)

        def add(numer, normer, j, log_weight):
            key = kvb[j, :, h * dqk : (h + 1) * dqk]
            value = kvb[j, :, qk + h * dv : qk + (h + 1) * dv]
            scores = lax.dot_general(
                query, key, (((1,), (1,)), ((), ())), preferred_element_type=jnp.float32
            )
            scores = scores * dqk ** (-0.5) * jnp.exp(log_weight - row_peak)
            high = scores.astype(low)
            rest = (scores - high.astype(jnp.float32)).astype(low)
            numer = (
                numer
                + jnp.dot(high, value, preferred_element_type=jnp.float32)
                + jnp.dot(rest, value, preferred_element_type=jnp.float32)
            )
            return numer, normer + jnp.sum(scores, axis=1, keepdims=True)

        numer, normer = add(numer, normer, s, pair)
        for j in range(n - 1):
            numer, normer = add(numer, normer, j, decay_col + weigh[j])
        cell = numer / jnp.maximum(jnp.abs(normer), jnp.exp(-row_peak))
        square = square + jnp.sum(cell * cell, axis=1, keepdims=True)
        span = slice(h * dv, (h + 1) * dv)
        gate = 1.0 / (1.0 + jnp.exp(-ogb[:, span].astype(jnp.float32)))
        gated.append((cell * hg_ref[:, span] * gate).astype(low))
    heads_out = jnp.concatenate(gated, axis=1)
    square_row = jnp.sum(jnp.where(eye, square, 0.0), axis=0, keepdims=True)
    sqb[t] = jnp.broadcast_to(square_row, sqb.shape[1:])
    for ox in range(2):
        for oc in range(2):
            if ox or oc:
                square_at = lambda: sqb.at[t]
                begin("all", ("sq", ox, oc), square_at, square_at, to(0, 0, ox, oc))

    def mixer_part(ox, oc):
        j = xs[ox] * 2 + oc
        cols = pl.ds(pl.multiple_of(j * width, width), width)
        pb[2 * ox + oc] = jnp.dot(
            heads_out, wob[:, cols], preferred_element_type=jnp.float32
        ).astype(low)

    def plus(ref, other):
        ref[...] = (ref[...].astype(jnp.float32) + other[...].astype(jnp.float32)).astype(low)

    x_at = lambda oz, oe, ox, ty: xb.at[places_z[oz], ys[oe], places_x[ox][ty]]

    @when("other")
    def _():
        for ox in (1, 0):
            for oc in range(2):
                mixer_part(ox, oc)
                begin(
                    "other", ("pc", ox, oc), lambda i=2 * ox + oc: pb.at[i],
                    lambda i=2 * ox + oc: spot(("pc", i)), to(0, 0, 0, 1),
                )

    hops = {"out": (1, 0, 0), "in": (3, 0, 0), "y": (0, 1, 0), "x": (0, 0, 1)}

    def forward(branch, oz, oe, ox, ty, way):
        tz, te, tx = hops[way]
        key = ("x", ty, oz ^ tz, oe ^ te, ox ^ tx)
        ref = lambda: x_at(oz, oe, ox, ty)
        begin(branch, key, ref, ref, to(tz, te, tx), way)

    def x_in(oz, oe, ox, ty):
        arrive(("x", ty, oz, oe, ox), x_at(oz, oe, ox, ty))

    @pl.when(lead)
    def _():
        for oc in range(2):
            mixer_part(1, oc)
            arrive(("pc", 1, oc), spot(("pc", 2 + oc)))
            plus(pb.at[2 + oc], spot(("pc", 2 + oc)))
            begin(
                "lead", ("px", oc), lambda i=2 + oc: pb.at[i], lambda oc=oc: pxb.at[oc],
                to(0, 0, 1),
            )
        for oc in range(2):
            mixer_part(0, oc)
            arrive(("pc", 0, oc), spot(("pc", oc)))
            plus(pb.at[oc], spot(("pc", oc)))
        arrive(("st",), stb.at[1 - c])

    for ox in range(2):
        for oc in range(2):
            if ox or oc:
                arrive(("sq", ox, oc), sqb.at[xs[ox] * 2 + cs[oc]])

    @pl.when(lead)
    def _():
        total_sq = to_column(jnp.sum(sqb[...], axis=0)[0:1])
        row_scale = lax.rsqrt(total_sq / (m * width) + norm_eps)
        for oc in (1, 0):
            arrive(("px", oc), pxb.at[oc])
            mixer = (pb[oc].astype(jnp.float32) + pxb[oc].astype(jnp.float32)) * row_scale
            own = x_at(0, 0, 0, oc)
            own[...] = (stb[oc].astype(jnp.float32) + mixer).astype(low)


            @when("lead mid")
            def _():
                forward("lead mid", 0, 0, 0, oc, "in")

            for way in ("out", "y", "x"):
                forward("lead", 0, 0, 0, oc, way)
        begin(
            "lead", ("res",), lambda: xb.at[places_z[0], y, cores[0][1]], lambda: resb, to(0, 0, 0, 1)
        )
        resb[...] = xb[places_z[0], y, cores[0][0]]

    def pass_on(branch, oz, way):
        for ty in (1, 0):
            x_in(oz, 0, 0, ty)

            @when(branch + " mid")
            def _():
                forward(branch + " mid", oz, 0, 0, ty, way)

            for turn in ("y", "x"):
                forward(branch, oz, 0, 0, ty, turn)

    @when("other")
    def _():
        pass_on("other", 1, "in")

        @pl.when(z == 0)
        def _():
            note_partner(0)

    @when("lead")
    def _():
        @pl.when(z == 0)
        def _():
            pl.semaphore_wait(note.at[0], 1)

    issue(3)

    for copy in load_own:
        copy.wait()

    def share(oz, oe):
        k = at(oz, oe)
        if oz or oe:
            arrive(("gu", oz, oe), gu_at(k))
        begin("all", ("gus", oz, oe), lambda: gu_at(k), lambda: gu_at(k), to(0, 0, 0, 1))

    def share_d(oz, oe):
        k = quarters[oz][oe]
        if oz or oe:
            arrive(("d", oz, oe), d_at(k))
        begin("all", ("ds", oz, oe), lambda: d_at(k), lambda: d_at(k), to(0, 0, 0, 1))

    @when("lead")
    def _():
        pass_on("lead", 2, "out")

    @when("other")
    def _():
        pass_on("other", 3, "out")

    for oz, oe in near:
        weights_d(oz, oe)
    share(0, 0)
    for oz, oe in near:
        share(oz, oe)

    for oz, oe in far[:2]:
        share(oz, oe)

    def turn_x(branch, zones):
        for oz in zones:
            for ty in (1, 0):
                x_in(oz, 1, 0, ty)
                forward(branch, oz, 1, 0, ty, "x")
        for oe in range(2):
            for oz in zones:
                for ty in (1, 0):
                    x_in(oz, oe, 1, ty)

    @when("lead")
    def _():
        turn_x("lead", (0, 2))

    @when("other")
    def _():
        turn_x("other", (1, 3))

    for oz, oe in far[2:]:
        share(oz, oe)
    share_d(0, 0)
    for oz, oe in near:
        share_d(oz, oe)
    for oz, oe in [(0, 0)] + near + far:
        arrive(("gus", oz, oe), gub.at[at(oz, oe), :, 1 - c, :part])

    nt = (((1,), (1,)), ((), ()))
    per = width // depth
    wide = 2 * room

    zone = z // 2

    def gate(i):
        size = 2 * rows
        squares = jnp.zeros((size, 1), jnp.float32)
        for j in range(m):
            piece = xb[i, :, j].reshape(size, width).astype(jnp.float32)
            squares = squares + jnp.sum(piece * piece, axis=1, keepdims=True)
        scale = lax.rsqrt(squares / (m * width) + norm_eps)
        act = jnp.zeros((size, 2 * wide), jnp.float32)
        for k in range(n):
            j, a = k // per, (k % per) * depth
            piece = xb[i, :, j, :, a : a + depth].reshape(size, depth).astype(jnp.float32)
            normed = (piece * scale * fg_ref[:, k * depth : (k + 1) * depth]).astype(low)
            act += lax.dot_general(
                normed, gub[k].reshape(2 * wide, depth), nt, preferred_element_type=jnp.float32
            )
        gate_act, up_act = act[:, :wide], act[:, wide:]
        hb[i, zone] = (gate_act / (1.0 + jnp.exp(-gate_act)) * up_act).astype(low)
        ref = lambda: hb.at[i, zone]
        begin("all", ("hid", i), ref, ref, to(2))

    def down(i):
        arrive(("hid", i), hb.at[i, 1 - zone])
        for k in range(n // 2):
            total = jnp.zeros((2 * rows, depth), jnp.float32)
            for w in range(2):
                total += jnp.dot(
                    hb[i, w], db[k, w].reshape(wide, depth), preferred_element_type=jnp.float32
                )
            j, a = k // per, (k % per) * depth
            ob[i, :, j, :, a : a + depth] = total.astype(low).reshape(2, rows, depth)

    gate(0)
    gate(1)
    for oz, oe in [(0, 0)] + near:
        arrive(("ds", oz, oe), db.at[quarters[oz][oe], :, 1 - c, :part])

    o_at = lambda oz, oe, ty: ob.at[places_z[oz], ys[oe], ty]

    def give(branch, stage, oz, oe, ty, way):
        tz, te, tx = hops[way]
        key = (stage, oz ^ tz, oe ^ te, ty)
        place = (stage, (oz ^ tz) // 2, oe ^ te, ty)
        begin(branch, key, lambda: o_at(oz, oe, ty), lambda: spot(place), to(tz, te, tx))

    def take(stage, oz, oe, ty):
        key, got = (stage, oz, oe, ty), spot((stage, oz // 2, oe, ty))
        arrive(key, got)
        plus(o_at(oz, oe, ty), got)

    def start(branch, oz):
        give(branch, "ry", oz, 1, 0, "y")
        if branch == "other":
            for oe in (1, 0):
                give(branch, "rz", oz, oe, 1, "out")

    for i in range(2):
        down(i)

        @when("lead")
        def _():
            for oz in (0, 2):

                @pl.when(places_z[oz] == i)
                def _():
                    start("lead", oz)

        @when("other")
        def _():
            for oz in (1, 3):

                @pl.when(places_z[oz] == i)
                def _():
                    start("other", oz)

    @when("other")
    def _():
        for oz in (3, 1):
            take("ry", oz, 0, 0)
            give("other", "rz", oz, 0, 0, "out")

    @when("lead")
    def _():
        for oz in (2, 0):
            take("rz", oz, 1, 1)
            give("lead", "ry", oz, 1, 1, "y")
            take("ry", oz, 0, 0)
            take("rz", oz, 0, 1)
        for oz in (2, 0):
            for ty in range(2):
                take("rz" if ty == 0 else "ry", oz, 0, ty)

                @when("lead away")
                def _():
                    give("lead away", "rx", oz, 0, ty, "x")

                @when("lead home")
                def _():
                    take("rx", oz, 0, ty)
                    if oz:
                        target = (at(2, 0), places_x[0][ty])
                        begin(
                            "lead home", ("rf", ty), lambda ty=ty: o_at(2, 0, ty),
                            lambda: spot(("rf",)), target,
                        )

        @when("lead home")
        def _():
            begin(
                "lead home", ("base",), lambda: ob.at[places_z[0], y, 1 - c],
                lambda: spot(("rf",)), to(0, 0, 0, 1),
            )
            spot(("rf",))[...] = ob[places_z[0], y, c]

    @when("other")
    def _():
        arrive(("res",), resb)

        @pl.when(home)
        def _():
            arrive(("base",), spot(("rf",)))

    @pl.when(jnp.logical_not(home))
    def _():
        for ty in range(2):

            @pl.when(c == ty)
            def _():
                arrive(("rf", ty), spot(("rf",)))

    total = resb[...].astype(jnp.float32) + spot(("rf",))[...].astype(jnp.float32)
    out_ref[...] = total.astype(low)

    for branch, condition in branches.items():

        def finish(branch=branch):
            for make in begun.get(branch, {}).values():
                make().wait_send()

        if condition is None:
            finish()
        else:
            pl.when(condition)(finish)


def fused(
    n, m, stream, queries, keys, values, out_gate, input_gate, forget_gate, head_gain, w_out,
    ffn_gain, w_gate, w_up, w_down,
):
    rows, width = stream.shape
    heads = input_gate.shape[1]
    depth, hidden = w_gate.shape
    part = hidden // n
    room = -(-part // 64) * 64
    low = jnp.bfloat16
    dma = pltpu.SemaphoreType.DMA
    vmem = pl.BlockSpec(memory_space=pltpu.VMEM)
    hbm = pl.BlockSpec(memory_space=pl.ANY)
    buffer = lambda *shape: pltpu.VMEM(shape, low)
    piece = (rows, width)
    return pl.pallas_call(
        functools.partial(fused_kernel, n, m, heads),
        out_shape=jax.ShapeDtypeStruct(piece, low),
        in_specs=[hbm] * 5 + [vmem] * 3 + [hbm, vmem] + [hbm] * 3,
        out_specs=vmem,
        scratch_shapes=[
            buffer(n, rows, keys.shape[1] + values.shape[1]),
            pltpu.VMEM((n, 2, heads, rows), jnp.float32),
            buffer(2, *piece),
            buffer(*queries.shape),
            buffer(*out_gate.shape),
            buffer(*w_out.shape),
            buffer(*w_gate.shape),
            buffer(*w_up.shape),
            buffer(n, 2, part, depth),
            buffer(n, 2, 2, room, depth),
            buffer(n // 2, 2, 2, room, depth),
            buffer(m, *piece),
            buffer(2, *piece),
            buffer(n // 4, 2, m, *piece),
            buffer(2, 2, 2 * rows, 2 * room),
            buffer(n // 4, 2, 2, *piece),
            buffer(SUMS, *piece),
            pltpu.VMEM((m, 8, rows), jnp.float32),
            buffer(*piece),
            dma((COPIES,)),
            dma((COPIES,)),
            dma((16,)),
            pltpu.SemaphoreType.REGULAR((2,)),
        ],
        compiler_params=pltpu.CompilerParams(
            collective_id=0, has_side_effects=True, vmem_limit_bytes=60 * 2**20
        ),
    )(
        stream, queries, keys, values, out_gate, forget_gate.T, input_gate.T,
        head_gain.reshape(1, -1), w_out, ffn_gain.reshape(1, -1), w_gate, w_up,
        w_down.reshape(2, n // 2, part, depth),
    )


def fits(n, m, stream, input_gate, w_gate):
    rows, width = stream.shape
    depth, hidden = w_gate.shape
    shaped = n // 2 == 4 and n % 2 == 0 and m == 4
    tiled = hidden % (16 * n) == 0 and hidden % 128 == 0 and depth % 128 == 0
    even = width % depth == 0 and rows == 128 and m * width == n * depth
    held = rows * width * 2 * 80 + 24 * depth * hidden
    return shaped and tiled and even and input_gate.shape[1] <= 4 and held < 40 * 2**20


def body(n, m, *arrays):
    if fits(n, m, arrays[0], arrays[5], arrays[10]):
        return fused(n, m, *arrays)
    return local(*arrays)


def solution(mesh):
    in_specs = (
        P("sp", "tp"),
        P("sp", "tp"),
        P("sp", "tp"),
        P("sp", "tp"),
        P("sp", "tp"),
        P("sp", "tp"),
        P("sp", "tp"),
        P("tp"),
        P("tp", None),
        P(),
        P("sp", "tp"),
        P("sp", "tp"),
        P("tp", "sp"),
    )
    out_specs = P("sp", "tp")
    each = functools.partial(body, mesh.shape["sp"], mesh.shape["tp"])
    return jax.shard_map(each, mesh=mesh, in_specs=in_specs, out_specs=out_specs, check_vma=False)
```

```python
import functools

import jax
import jax.numpy as jnp
from jax import lax
from jax.experimental import pallas as pl
from jax.experimental.pallas import tpu as pltpu
from jax.sharding import PartitionSpec as P

D = 2048
DQK = 128
DV = 256
BLOCK = 64
VALS = 2048


precise = lax.Precision.HIGHEST
norm_eps = 1e-06
very_low = -1e30


def entering(value, axis, join, neutral):
    count, mine = (lax.axis_size(axis), lax.axis_index(axis))
    pieces = jax.tree.map(lambda part: lax.all_gather(part, axis), value)
    subtotal = jax.tree.map(
        lambda part, zero: jnp.full_like(part, 0) + jnp.asarray(zero, part.dtype), value, neutral
    )

    def step(position, subtotal):
        longer = join(subtotal, jax.tree.map(lambda part: part[position], pieces))
        return jax.tree.map(lambda new, old: jnp.where(position < mine, new, old), longer, subtotal)

    return lax.fori_loop(0, count - 1, step, subtotal)


def block_summary(key_blk, value_blk, input_blk, decay_sum):
    decay_total = decay_sum[..., -1]
    log_weight = decay_total[..., None] - decay_sum + input_blk
    weight_peak = jnp.max(log_weight, axis=-1)
    weights = jnp.exp(log_weight - weight_peak[..., None])
    state_mat = jnp.einsum(
        "...ld,...le->...de", weights[..., None] * key_blk, value_blk, precision=precise
    )
    state_vec = jnp.einsum("...l,...ld->...d", weights, key_blk, precision=precise)
    return (state_mat, state_vec, weight_peak, decay_total)


def combine(earlier, later):
    ceiling = jnp.maximum(later[3] + earlier[2], later[2])
    former = jnp.exp(later[3] + earlier[2] - ceiling)
    latter = jnp.exp(later[2] - ceiling)
    return (
        former[..., None, None] * earlier[0] + latter[..., None, None] * later[0],
        former[..., None] * earlier[1] + latter[..., None] * later[1],
        ceiling,
        earlier[3] + later[3],
    )


def block_output(
    query_blk, key_blk, value_blk, input_blk, decay_sum, state_mat, state_vec, state_peak
):
    block_len = query_blk.shape[-2]
    causal = jnp.tril(jnp.ones((block_len, block_len), jnp.bool_))
    log_pair = jnp.where(
        causal,
        decay_sum[..., :, None] - decay_sum[..., None, :] + input_blk[..., None, :],
        -jnp.inf,
    )
    log_carry = decay_sum + state_peak[..., None]
    row_peak = jnp.maximum(log_carry, jnp.max(log_pair, axis=-1))
    scores = jnp.einsum("...ld,...sd->...ls", query_blk, key_blk, precision=precise) * jnp.exp(
        log_pair - row_peak[..., None]
    )
    carried = jnp.exp(log_carry - row_peak)
    numer = jnp.einsum("...ls,...se->...le", scores, value_blk, precision=precise) + carried[
        ..., None
    ] * jnp.einsum("...ld,...de->...le", query_blk, state_mat, precision=precise)
    normer = jnp.sum(scores, axis=-1) + carried * jnp.einsum(
        "...ld,...d->...l", query_blk, state_vec, precision=precise
    )
    denom = jnp.maximum(jnp.abs(normer), jnp.exp(-row_peak))
    return numer / denom[..., None]


def local(
    stream,
    queries,
    keys,
    values,
    out_gate,
    input_gate,
    forget_gate,
    head_gain,
    w_out,
    ffn_gain,
    w_gate,
    w_up,
    w_down,
):
    gate_full, up_full, down_full = (
        lax.all_gather(w_gate, "sp", axis=0, tiled=True),
        lax.all_gather(w_up, "sp", axis=0, tiled=True),
        lax.all_gather(w_down, "sp", axis=1, tiled=True),
    )
    count_of_rows = stream.shape[0]
    head_count = input_gate.shape[1]
    blocks = count_of_rows // BLOCK

    def to_blocks(array, col_width):
        return (
            array.astype(jnp.float32)
            .reshape(blocks, BLOCK, head_count, col_width)
            .transpose(2, 0, 1, 3)
        )

    query_blk = to_blocks(queries, DQK) * DQK ** (-0.5)
    key_blk = to_blocks(keys, DQK)
    value_blk = to_blocks(values, DV)
    input_blk = input_gate.reshape(blocks, BLOCK, head_count).transpose(2, 0, 1)
    decay_sum = jnp.cumsum(
        jax.nn.log_sigmoid(forget_gate).reshape(blocks, BLOCK, head_count).transpose(2, 0, 1),
        axis=-1,
    )
    summary = block_summary(key_blk, value_blk, input_blk, decay_sum)
    identity = (
        jnp.zeros((head_count, DQK, DV), jnp.float32),
        jnp.zeros((head_count, DQK), jnp.float32),
        jnp.full((head_count,), very_low, jnp.float32),
        jnp.zeros((head_count,), jnp.float32),
    )

    def advance(carry, piece):
        return (combine(carry, piece), carry)

    local_total, prefix = lax.scan(
        advance, identity, jax.tree.map(lambda array: jnp.moveaxis(array, 1, 0), summary)
    )
    carry_in = entering(local_total, "sp", combine, identity)
    start = combine(
        jax.tree.map(lambda array: array[:, None], carry_in),
        jax.tree.map(lambda array: jnp.moveaxis(array, 0, 1), prefix),
    )
    mixed_heads = block_output(
        query_blk, key_blk, value_blk, input_blk, decay_sum, start[0], start[1], start[2]
    )
    head_rows = mixed_heads.transpose(1, 2, 0, 3).reshape(count_of_rows, head_count, DV)
    local_sq = jnp.sum(head_rows * head_rows, axis=(1, 2))
    total_sq = lax.psum(local_sq, "tp")
    row_scale = lax.rsqrt(total_sq / VALS + norm_eps)
    gated = (
        head_rows
        * row_scale[:, None, None]
        * head_gain.reshape(head_count, DV)
        * jax.nn.sigmoid(out_gate.astype(jnp.float32).reshape(count_of_rows, head_count, DV))
    )
    heads_out = gated.reshape(count_of_rows, head_count * DV).astype(jnp.bfloat16)
    partial_value = jnp.dot(heads_out, w_out, preferred_element_type=jnp.float32)
    col_width = stream.shape[1]
    col_start = lax.axis_index("tp") * col_width
    mixer_own = lax.psum_scatter(
        partial_value.astype(jnp.bfloat16), "tp", scatter_dimension=1, tiled=True
    ).astype(jnp.float32)
    resid_own = (stream.astype(jnp.float32) + mixer_own).astype(jnp.bfloat16)
    resid_f = resid_own.astype(jnp.float32)
    square_total = lax.psum(jnp.sum(resid_f * resid_f, axis=-1), "tp")
    gain_own = lax.dynamic_slice_in_dim(ffn_gain, col_start, col_width)
    normed_own = (resid_f * lax.rsqrt(square_total / D + norm_eps)[:, None] * gain_own).astype(
        jnp.bfloat16
    )
    normed = lax.all_gather(normed_own, "tp", axis=1, tiled=True)
    gate_act = jnp.dot(normed, gate_full, preferred_element_type=jnp.float32)
    up_act = jnp.dot(normed, up_full, preferred_element_type=jnp.float32)
    hidden = (jax.nn.silu(gate_act) * up_act).astype(jnp.bfloat16)
    term = jnp.dot(hidden, down_full, preferred_element_type=jnp.float32)
    down_own = lax.psum_scatter(
        term.astype(jnp.bfloat16), "tp", scatter_dimension=1, tiled=True
    ).astype(jnp.float32)
    return (resid_own.astype(jnp.float32) + down_own).astype(jnp.bfloat16)


def remote(src, dst, send, recv, target):
    return pltpu.make_async_remote_copy(
        src_ref=src,
        dst_ref=dst,
        send_sem=send,
        recv_sem=recv,
        device_id=target,
        device_id_type=pl.DeviceIdType.MESH,
    )


COPIES = 256
SUMS = 28


def fused_kernel(
    n, m, heads, stream_h, q_h, k_h, v_h, og_h, f_h, i_h, hg_h, wo_h, fg_h, wg_h, wu_h, wd_h,
    out_ref, f_ref, i_ref, hg_ref, fg_ref, kvb, gb, stb, qb, ogb, wob, wgb, wub, wtb, gub, db, pb, pxb, xb, hb, ob, rb, sqb,
    resb, ssem, rsem, lsem, note,
):
    rows, width = out_ref.shape
    ring = n // 2
    half = rows // 2
    dv = width // heads
    dqk = qb.shape[1] // heads
    part, depth = wtb.shape[2], wtb.shape[3]
    room = gub.shape[3]
    low = jnp.bfloat16
    s, t = lax.axis_index("sp"), lax.axis_index("tp")
    z, y, x, c = s // 2, s % 2, t // 2, t % 2
    lead, middle = z % 2 == c, (z == 1) | (z == 2)
    zs = [2 * ((z // 2 + d // 2) % 2) + (z + d) % 2 for d in range(ring)]
    ys, xs, cs = ([y, 1 - y], [x, 1 - x], [c, 1 - c])
    ranks = [[zs[oz] * 2 + ys[oe] for oe in range(2)] for oz in range(ring)]
    cores = [[xs[ox] * 2 + cs[oc] for oc in range(2)] for ox in range(2)]
    places_x = [[xs[ox] * 2 + ty for ty in range(2)] for ox in range(2)]
    places_z = [v // 2 for v in zs]
    at = lambda oz, oe: ranks[oz][oe]
    to = lambda oz=0, oe=0, ox=0, oc=0: (at(oz, oe), cores[ox][oc])
    under = [[(z + ring - d) % ring * 2 + ys[oe] for oe in range(2)] for d in range(ring)]
    above = ((z + 1) % ring * 2 + y, t)
    home = x == z // 2
    branches = {
        "all": None,
        "lead home": lead & home,
        "lead away": lead & jnp.logical_not(home),
        "lead": lead,
        "other": jnp.logical_not(lead),
        "lead0": lead & (c == 0),
        "lead1": lead & (c == 1),
        "lead mid": lead & middle,
        "other one": jnp.logical_not(lead) & (z == 1),
        "other two": jnp.logical_not(lead) & (z == 2),
        "other end": jnp.logical_not(lead | middle),
        "lead end": lead & jnp.logical_not(middle),
        "low y": y == 0,
        "lower": z < 2,
        "upper": z >= 2,
    }
    for d in range(ring):
        branches["at", d] = z == d
        branches["from", d] = z >= d
        branches["up", d] = (z >= d) & (z < ring - 1)

    def when(branch):
        return pl.when(branches[branch])

    first, second = slice(0, half), slice(half, rows)
    places, begun, spots = {}, {}, {}

    def place(key):
        i = places.setdefault(key, len(places))
        assert i < COPIES
        return i

    def begin(branch, key, src, dst, target, tag=""):
        def make():
            return remote(
                src(), dst(), ssem.at[place((key, tag))], rsem.at[place((key, ""))], target
            )

        make().start()
        begun.setdefault(branch, {})[key, tag] = make

    def arrive(key, ref):
        i = place((key, ""))
        remote(ref, ref, ssem.at[i], rsem.at[i], to(0, 0, 0, 1)).wait_recv()

    def spot(key):
        i = spots.setdefault(key, len(spots))
        assert i < SUMS
        return rb.at[i]

    count = [0]

    def local(src, dst):
        copy = pltpu.make_async_copy(src, dst, lsem.at[count[0]])
        count[0] += 1
        copy.start()
        return copy

    qk = heads * dqk
    load_kv = [local(k_h, kvb.at[s, :, :qk]), local(v_h, kvb.at[s, :, qk:])]
    load_w = [local(wg_h, wgb), local(wu_h, wub)]
    load_f = [local(f_h, f_ref), local(i_h, i_ref)]
    load_g = [local(f_h, gb.at[s, 0]), local(i_h, gb.at[s, 1])]
    load_gain = [local(hg_h, hg_ref), local(fg_h, fg_ref)]
    load_cell = [local(q_h, qb), local(og_h, ogb)]
    load_rest = [local(wo_h, wob), local(stream_h, stb.at[c])]

    barrier = pltpu.get_barrier_semaphore()
    peers = [to(oz, oe) for oz in range(ring) for oe in range(2) if oz or oe]
    peers += [to(0, 0, ox, oc) for ox in range(2) for oc in range(2) if ox or oc]
    peers += [to(1, 0, 0, 1), to(2, 0, 0, 1)]
    for peer in peers:
        pl.semaphore_signal(barrier, inc=1, device_id=peer, device_id_type=pl.DeviceIdType.MESH)
    pl.semaphore_wait(barrier, len(peers))

    for copy in load_f:
        copy.wait()
    others = [(oz, oe) for oz in range(ring) for oe in range(2) if oz or oe]
    for oz, oe in others:
        for w, ref in enumerate((f_ref, i_ref)):
            begin(
                "all", ("g", w, oz, oe), lambda ref=ref: ref, lambda w=w: gb.at[s, w],
                to(oz, oe),
            )

    def piece_kv(d, oe, rows_of):
        return kvb.at[under[d][oe]].at[rows_of]

    def kv(branch, d, way, rows_of):
        up = way == "up"
        key = ("kv", d + up, 1 - up, rows_of is second)
        ref = lambda: piece_kv(d, 0, rows_of)
        begin(branch, key, ref, ref, above if up else to(0, 1))

    def kv_in(d, oe, rows_of):
        arrive(("kv", d, oe, rows_of is second), piece_kv(d, oe, rows_of))

    for copy in load_kv:
        copy.wait()

    for rows_of in (first, second):

        @when(("up", 0))
        def _():
            kv(("up", 0), 0, "up", rows_of)

        @when("low y")
        def _():
            kv("low y", 0, "across", rows_of)

    for j in range(1, n - 1):

        @pl.when(j > s)
        def _():
            kvb[j] = jnp.zeros(kvb.shape[1:], low)

    zero = jnp.zeros((room - part, depth), low)
    for k in range(n):
        for core in range(2):
            for w in range(2):
                gub[k, w, core, part:] = zero
                if k < n // 2:
                    db[k, w, core, part:] = zero
    for copy in load_w:
        copy.wait()
    lanes = 128
    for w, source in enumerate((wgb, wub)):
        for q in range(source.shape[1] // lanes):
            turned = source[:, q * lanes : (q + 1) * lanes].T
            cut = q * lanes
            while cut < (q + 1) * lanes:
                stop = min((cut // part + 1) * part, (q + 1) * lanes)
                off = cut % part
                wtb[cut // part, w, off : off + stop - cut] = turned[cut - q * lanes : stop - q * lanes]
                cut = stop

    gu_at = lambda k: gub.at[k, :, c, :part]
    d_at = lambda k: db.at[k, :, c, :part]

    def weights(branch, oz, oe):
        k = at(oz, oe)
        begin(branch, ("gu", oz, oe), lambda: wtb.at[k], lambda: gu_at(s), to(oz, oe))

    quarters = [[zs[oz] % 2 * 2 + ys[oe] for oe in range(2)] for oz in range(2)]
    mine = quarters[0][0]

    def weights_d(oz, oe):
        k = quarters[oz][oe]
        begin("all", ("d", oz, oe), lambda: wd_h.at[:, k], lambda: d_at(mine), to(oz, oe))

    load_own = [local(wtb.at[s], gu_at(s)), local(wd_h.at[:, mine], d_at(mine))]

    near = [(0, 1), (1, 0), (1, 1)]
    far = [(2, 0), (3, 0), (2, 1), (3, 1)]
    plan = {
        0: ([(1, 0), (0, 1)], [], [], [(2, 0), (2, 1), (3, 0), (3, 1), (1, 1)], []),
        1: ([(1, 0)], [(3, 0), (3, 1)], [], [(2, 0), (2, 1), (0, 1), (1, 1)], []),
        2: ([(3, 0), (2, 0)], [], [(1, 0), (3, 1)], [(2, 1), (0, 1)], [(1, 1)]),
        3: ([(2, 0), (3, 0), (1, 0)], [], [(2, 1)], [(3, 1), (0, 1), (1, 1)], []),
    }

    def issue(phase):
        for at_z, phases in plan.items():
            if phases[phase]:

                @when(("at", at_z))
                def _():
                    for oz, oe in phases[phase]:
                        weights(("at", at_z), oz, oe)

    issue(0)

    for d in range(1, ring):
        for rows_of in (first, second):

            @when(("from", d))
            def _():
                kv_in(d, 0, rows_of)
                if d < ring - 1:

                    @when(("up", d))
                    def _():
                        kv(("up", d), d, "up", rows_of)

                kv(("from", d), d, "across", rows_of)

    note_partner = lambda i: pl.semaphore_signal(
        note.at[i], inc=1, device_id=to(0, 0, 0, 1), device_id_type=pl.DeviceIdType.MESH
    )
    note_partner(1)
    pl.semaphore_wait(note.at[1], 1)

    issue(1)

    for rows_of in (first, second):

        @pl.when(y == 1)
        def _():
            kv_in(0, 1, rows_of)

        for d in range(1, ring):

            @when(("from", d))
            def _():
                kv_in(d, 1, rows_of)

    issue(2)
    for oz, oe in others:
        for w in range(2):
            arrive(("g", w, oz, oe), gb.at[at(oz, oe), w])
    for copy in load_cell + load_g + load_gain + load_rest:
        copy.wait()

    @when("other")
    def _():
        begin("other", ("st",), lambda: stb.at[c], lambda: stb.at[c], to(0, 0, 0, 1))

    at_row = lax.broadcasted_iota(jnp.int32, (rows, rows), 0)
    at_col = lax.broadcasted_iota(jnp.int32, (rows, rows), 1)
    eye, causal = at_row == at_col, at_row >= at_col
    to_column = lambda row: jnp.sum(jnp.where(eye, row, 0.0), axis=1, keepdims=True)
    upper = (at_row <= at_col).astype(jnp.float32)
    gates = jnp.concatenate([gb[j, 0] for j in range(n)], axis=0)
    entries = jnp.concatenate([gb[j, 1] for j in range(n)], axis=0)
    log_sigmoid = lambda v: jnp.minimum(v, 0.0) - jnp.log1p(jnp.exp(-jnp.abs(v)))
    decays = jnp.dot(
        log_sigmoid(gates), upper, precision=precise, preferred_element_type=jnp.float32
    )
    own_decay = jnp.dot(
        log_sigmoid(f_ref[...]), upper, precision=precise, preferred_element_type=jnp.float32
    )
    own_entry = i_ref[...]
    square = jnp.zeros((rows, 1), jnp.float32)
    gated = []
    for h in range(heads):
        decay_row = own_decay[h : h + 1]
        decay_col = to_column(decay_row)
        after = jnp.zeros((1, 1), jnp.float32)
        peak = jnp.full((1, 1), very_low, jnp.float32)
        weigh = [None] * n
        for j in reversed(range(n)):
            earlier = j < s
            block = decays[j * heads + h : j * heads + h + 1]
            total = block[:, rows - 1 :]
            entry = entries[j * heads + h : j * heads + h + 1]
            weigh[j] = jnp.where(earlier, total - block + entry + after, very_low)
            after = after + jnp.where(earlier, total, 0.0)
            peak = jnp.maximum(peak, jnp.max(weigh[j], axis=1, keepdims=True))
        pair = jnp.where(causal, decay_col - decay_row + own_entry[h : h + 1], very_low)
        row_peak = jnp.maximum(decay_col + peak, jnp.max(pair, axis=1, keepdims=True))
        query = qb[:, h * dqk : (h + 1) * dqk]
        numer = jnp.zeros((rows, dv), jnp.float32)
        normer = jnp.zeros((rows, 1), jnp.float32)

        def add(numer, normer, j, log_weight):
            key = kvb[j, :, h * dqk : (h + 1) * dqk]
            value = kvb[j, :, qk + h * dv : qk + (h + 1) * dv]
            scores = lax.dot_general(
                query, key, (((1,), (1,)), ((), ())), preferred_element_type=jnp.float32
            )
            scores = scores * dqk ** (-0.5) * jnp.exp(log_weight - row_peak)
            high = scores.astype(low)
            rest = (scores - high.astype(jnp.float32)).astype(low)
            numer = (
                numer
                + jnp.dot(high, value, preferred_element_type=jnp.float32)
                + jnp.dot(rest, value, preferred_element_type=jnp.float32)
            )
            return numer, normer + jnp.sum(scores, axis=1, keepdims=True)

        numer, normer = add(numer, normer, s, pair)
        for j in range(n - 1):
            numer, normer = add(numer, normer, j, decay_col + weigh[j])
        cell = numer / jnp.maximum(jnp.abs(normer), jnp.exp(-row_peak))
        square = square + jnp.sum(cell * cell, axis=1, keepdims=True)
        span = slice(h * dv, (h + 1) * dv)
        gate = 1.0 / (1.0 + jnp.exp(-ogb[:, span].astype(jnp.float32)))
        gated.append((cell * hg_ref[:, span] * gate).astype(low))
    heads_out = jnp.concatenate(gated, axis=1)
    square_row = jnp.sum(jnp.where(eye, square, 0.0), axis=0, keepdims=True)
    sqb[t] = jnp.broadcast_to(square_row, sqb.shape[1:])
    for ox in range(2):
        for oc in range(2):
            if ox or oc:
                square_at = lambda: sqb.at[t]
                begin("all", ("sq", ox, oc), square_at, square_at, to(0, 0, ox, oc))

    def mixer_part(ox, oc):
        j = xs[ox] * 2 + oc
        cols = pl.ds(pl.multiple_of(j * width, width), width)
        pb[2 * ox + oc] = jnp.dot(
            heads_out, wob[:, cols], preferred_element_type=jnp.float32
        ).astype(low)

    def plus(ref, other):
        ref[...] = (ref[...].astype(jnp.float32) + other[...].astype(jnp.float32)).astype(low)

    x_at = lambda oz, oe, ox, ty: xb.at[places_z[oz], ys[oe], places_x[ox][ty]]

    @when("other")
    def _():
        for ox in (1, 0):
            for oc in range(2):
                mixer_part(ox, oc)
                begin(
                    "other", ("pc", ox, oc), lambda i=2 * ox + oc: pb.at[i],
                    lambda i=2 * ox + oc: spot(("pc", i)), to(0, 0, 0, 1),
                )

    hops = {"out": (1, 0, 0), "in": (3, 0, 0), "y": (0, 1, 0), "x": (0, 0, 1)}

    def forward(branch, oz, oe, ox, ty, way):
        tz, te, tx = hops[way]
        key = ("x", ty, oz ^ tz, oe ^ te, ox ^ tx)
        ref = lambda: x_at(oz, oe, ox, ty)
        begin(branch, key, ref, ref, to(tz, te, tx), way)

    def spread(branch, oz, ty, ways):
        for way in ways:
            forward(branch, oz, 0, 0, ty, way)
        for turn in ("y", "x"):
            forward(branch, oz, 0, 0, ty, turn)

    def x_in(oz, oe, ox, ty):
        arrive(("x", ty, oz, oe, ox), x_at(oz, oe, ox, ty))

    @pl.when(lead)
    def _():
        for oc in range(2):
            mixer_part(1, oc)
            arrive(("pc", 1, oc), spot(("pc", 2 + oc)))
            plus(pb.at[2 + oc], spot(("pc", 2 + oc)))
            begin(
                "lead", ("px", oc), lambda i=2 + oc: pb.at[i], lambda oc=oc: pxb.at[oc],
                to(0, 0, 1),
            )
        for oc in range(2):
            mixer_part(0, oc)
            arrive(("pc", 0, oc), spot(("pc", oc)))
            plus(pb.at[oc], spot(("pc", oc)))
        arrive(("st",), stb.at[1 - c])

    for ox in range(2):
        for oc in range(2):
            if ox or oc:
                arrive(("sq", ox, oc), sqb.at[xs[ox] * 2 + cs[oc]])

    @pl.when(lead)
    def _():
        total_sq = to_column(jnp.sum(sqb[...], axis=0)[0:1])
        row_scale = lax.rsqrt(total_sq / (m * width) + norm_eps)
        for oc in (1, 0):
            arrive(("px", oc), pxb.at[oc])
            mixer = (pb[oc].astype(jnp.float32) + pxb[oc].astype(jnp.float32)) * row_scale
            own = x_at(0, 0, 0, oc)
            own[...] = (stb[oc].astype(jnp.float32) + mixer).astype(low)


            for branch, ways in (("lead mid", ("in", "out")), ("lead end", ("out",))):

                @when(branch)
                def _():
                    spread(branch, 0, oc, ways)


        begin(
            "lead", ("res",), lambda: xb.at[places_z[0], y, cores[0][1]], lambda: resb, to(0, 0, 0, 1)
        )
        resb[...] = xb[places_z[0], y, cores[0][0]]

    def pass_on(branch, oz, *ways):
        for ty in (1, 0):
            x_in(oz, 0, 0, ty)
            spread(branch, oz, ty, ways)

    @when("other end")
    def _():
        pass_on("other end", 1)

    @when("other two")
    def _():
        pass_on("other two", 3, "out")
        pass_on("other two", 1, "in")

    @when("other one")
    def _():
        pass_on("other one", 1, "in")
        for ty in (1, 0):
            begun["other one"].pop((("x", ty, 2, 0, 0), "in"))().wait_send()
        for oc in range(2):
            pl.semaphore_signal(
                note.at[0], inc=1, device_id=to(1, 0, 0, oc), device_id_type=pl.DeviceIdType.MESH
            )

    @when(("at", 0))
    def _():
        pl.semaphore_wait(note.at[0], 1)

    issue(3)


    for copy in load_own:
        copy.wait()

    def share(oz, oe):
        k = at(oz, oe)
        if oz or oe:
            arrive(("gu", oz, oe), gu_at(k))
        begin("all", ("gus", oz, oe), lambda: gu_at(k), lambda: gu_at(k), to(0, 0, 0, 1))

    def share_d(oz, oe):
        k = quarters[oz][oe]
        if oz or oe:
            arrive(("d", oz, oe), d_at(k))
        begin("all", ("ds", oz, oe), lambda: d_at(k), lambda: d_at(k), to(0, 0, 0, 1))

    @when("lead mid")
    def _():
        pass_on("lead mid", 2, "out")

    @when("lead end")
    def _():
        pass_on("lead end", 2)

    @when("other one")
    def _():
        pass_on("other one", 3, "out")

    @when("other end")
    def _():
        pass_on("other end", 3)

    issue(4)
    for oz, oe in near:
        weights_d(oz, oe)
    sides = {"lead": (0, 2), "other": (1, 3)}
    for role, zones in sides.items():

        @when(role)
        def _():
            for oz in zones:
                for ty in (1, 0):
                    x_in(oz, 1, 0, ty)
                    forward(role, oz, 1, 0, ty, "x")

    share(0, 0)
    for oz, oe in near:
        share(oz, oe)

    for oz, oe in far[:2]:
        share(oz, oe)

    for oz, oe in far[2:]:
        share(oz, oe)

    for role, zones in sides.items():

        @when(role)
        def _():
            for oz in zones:
                for oe in range(2):
                    for ty in (1, 0):
                        x_in(oz, oe, 1, ty)

    for oz, oe in [(0, 0)] + near + far:
        arrive(("gus", oz, oe), gub.at[at(oz, oe), :, 1 - c, :part])

    nt = (((1,), (1,)), ((), ()))
    per = width // depth
    wide = 2 * room

    zone = z // 2

    def gate(i):
        size = 2 * rows
        squares = jnp.zeros((size, 1), jnp.float32)
        for j in range(m):
            piece = xb[i, :, j].reshape(size, width).astype(jnp.float32)
            squares = squares + jnp.sum(piece * piece, axis=1, keepdims=True)
        scale = lax.rsqrt(squares / (m * width) + norm_eps)
        act = jnp.zeros((size, 2 * wide), jnp.float32)
        for k in range(n):
            j, a = k // per, (k % per) * depth
            piece = xb[i, :, j, :, a : a + depth].reshape(size, depth).astype(jnp.float32)
            normed = (piece * scale * fg_ref[:, k * depth : (k + 1) * depth]).astype(low)
            act += lax.dot_general(
                normed, gub[k].reshape(2 * wide, depth), nt, preferred_element_type=jnp.float32
            )
        gate_act, up_act = act[:, :wide], act[:, wide:]
        hb[i, zone] = (gate_act / (1.0 + jnp.exp(-gate_act)) * up_act).astype(low)
        ref = lambda: hb.at[i, zone]
        begin("all", ("hid", i), ref, ref, to(2))

    def down(i):
        arrive(("hid", i), hb.at[i, 1 - zone])
        for k in range(n // 2):
            total = jnp.zeros((2 * rows, depth), jnp.float32)
            for w in range(2):
                total += jnp.dot(
                    hb[i, w], db[k, w].reshape(wide, depth), preferred_element_type=jnp.float32
                )
            j, a = k // per, (k % per) * depth
            ob[i, :, j, :, a : a + depth] = total.astype(low).reshape(2, rows, depth)

    gate(0)
    gate(1)
    share_d(0, 0)
    for oz, oe in near:
        share_d(oz, oe)
    for oz, oe in [(0, 0)] + near:
        arrive(("ds", oz, oe), db.at[quarters[oz][oe], :, 1 - c, :part])

    o_at = lambda oz, oe, ty: ob.at[places_z[oz], ys[oe], ty]

    def give(branch, stage, oz, oe, ty, way):
        tz, te, tx = hops[way]
        key = (stage, oz ^ tz, oe ^ te, ty)
        place = (stage, (oz ^ tz) // 2, oe ^ te, ty)
        begin(branch, key, lambda: o_at(oz, oe, ty), lambda: spot(place), to(tz, te, tx))

    def take(stage, oz, oe, ty):
        key, got = (stage, oz, oe, ty), spot((stage, oz // 2, oe, ty))
        arrive(key, got)
        plus(o_at(oz, oe, ty), got)

    def start(branch, oz):
        give(branch, "ry", oz, 1, 0, "y")
        if branch == "other":
            for oe in (1, 0):
                give(branch, "rz", oz, oe, 1, "out")

    for i in range(2):
        down(i)

        @when("lead")
        def _():
            for oz in (0, 2):

                @pl.when(places_z[oz] == i)
                def _():
                    start("lead", oz)

        @when("other")
        def _():
            for oz in (1, 3):

                @pl.when(places_z[oz] == i)
                def _():
                    start("other", oz)

    @when("other")
    def _():
        for oz in (3, 1):
            take("ry", oz, 0, 0)
            give("other", "rz", oz, 0, 0, "out")

    @when("lead")
    def _():
        for oz in (2, 0):
            take("rz", oz, 1, 1)
            give("lead", "ry", oz, 1, 1, "y")
            take("ry", oz, 0, 0)
            take("rz", oz, 0, 1)
        for oz in (2, 0):
            for ty in range(2):
                take("rz" if ty == 0 else "ry", oz, 0, ty)

                @when("lead away")
                def _():
                    give("lead away", "rx", oz, 0, ty, "x")

                @when("lead home")
                def _():
                    take("rx", oz, 0, ty)
                    if oz:
                        target = (at(2, 0), places_x[0][ty])
                        begin(
                            "lead home", ("rf", ty), lambda ty=ty: o_at(2, 0, ty),
                            lambda: spot(("rf",)), target,
                        )

        @when("lead home")
        def _():
            begin(
                "lead home", ("base",), lambda: ob.at[places_z[0], y, 1 - c],
                lambda: spot(("rf",)), to(0, 0, 0, 1),
            )
            spot(("rf",))[...] = ob[places_z[0], y, c]

    @when("other")
    def _():
        arrive(("res",), resb)

        @pl.when(home)
        def _():
            arrive(("base",), spot(("rf",)))

    @pl.when(jnp.logical_not(home))
    def _():
        for ty in range(2):

            @pl.when(c == ty)
            def _():
                arrive(("rf", ty), spot(("rf",)))

    total = resb[...].astype(jnp.float32) + spot(("rf",))[...].astype(jnp.float32)
    out_ref[...] = total.astype(low)

    for branch, condition in branches.items():

        def finish(branch=branch):
            for make in begun.get(branch, {}).values():
                make().wait_send()

        if condition is None:
            finish()
        else:
            pl.when(condition)(finish)


def fused(
    n, m, stream, queries, keys, values, out_gate, input_gate, forget_gate, head_gain, w_out,
    ffn_gain, w_gate, w_up, w_down,
):
    rows, width = stream.shape
    heads = input_gate.shape[1]
    depth, hidden = w_gate.shape
    part = hidden // n
    room = -(-part // 64) * 64
    low = jnp.bfloat16
    dma = pltpu.SemaphoreType.DMA
    vmem = pl.BlockSpec(memory_space=pltpu.VMEM)
    hbm = pl.BlockSpec(memory_space=pltpu.HBM)
    buffer = lambda *shape: pltpu.VMEM(shape, low)
    piece = (rows, width)
    return pl.pallas_call(
        functools.partial(fused_kernel, n, m, heads),
        out_shape=jax.ShapeDtypeStruct(piece, low),
        in_specs=[hbm] * 13,
        out_specs=vmem,
        scratch_shapes=[
            pltpu.VMEM((heads, rows), jnp.float32),
            pltpu.VMEM((heads, rows), jnp.float32),
            pltpu.VMEM((1, head_gain.shape[0]), jnp.float32),
            pltpu.VMEM((1, ffn_gain.shape[0]), jnp.float32),
            buffer(n, rows, keys.shape[1] + values.shape[1]),
            pltpu.VMEM((n, 2, heads, rows), jnp.float32),
            buffer(2, *piece),
            buffer(*queries.shape),
            buffer(*out_gate.shape),
            buffer(*w_out.shape),
            buffer(*w_gate.shape),
            buffer(*w_up.shape),
            buffer(n, 2, part, depth),
            buffer(n, 2, 2, room, depth),
            buffer(n // 2, 2, 2, room, depth),
            buffer(m, *piece),
            buffer(2, *piece),
            buffer(n // 4, 2, m, *piece),
            buffer(2, 2, 2 * rows, 2 * room),
            buffer(n // 4, 2, 2, *piece),
            buffer(SUMS, *piece),
            pltpu.VMEM((m, 8, rows), jnp.float32),
            buffer(*piece),
            dma((COPIES,)),
            dma((COPIES,)),
            dma((20,)),
            pltpu.SemaphoreType.REGULAR((2,)),
        ],
        compiler_params=pltpu.CompilerParams(
            collective_id=0, has_side_effects=True, vmem_limit_bytes=60 * 2**20
        ),
    )(
        stream, queries, keys, values, out_gate, forget_gate.T, input_gate.T,
        head_gain.reshape(1, -1), w_out, ffn_gain.reshape(1, -1), w_gate, w_up,
        w_down.reshape(2, n // 2, part, depth),
    )


def fits(n, m, stream, input_gate, w_gate):
    rows, width = stream.shape
    depth, hidden = w_gate.shape
    shaped = n // 2 == 4 and n % 2 == 0 and m == 4
    tiled = hidden % (16 * n) == 0 and hidden % 128 == 0 and depth % 128 == 0
    even = width % depth == 0 and rows == 128 and m * width == n * depth
    held = rows * width * 2 * 80 + 24 * depth * hidden
    return shaped and tiled and even and input_gate.shape[1] <= 4 and held < 40 * 2**20


def body(n, m, *arrays):
    if fits(n, m, arrays[0], arrays[5], arrays[10]):
        return fused(n, m, *arrays)
    return local(*arrays)


def solution(mesh):
    in_specs = (
        P("sp", "tp"),
        P("sp", "tp"),
        P("sp", "tp"),
        P("sp", "tp"),
        P("sp", "tp"),
        P("sp", "tp"),
        P("sp", "tp"),
        P("tp"),
        P("tp", None),
        P(),
        P("sp", "tp"),
        P("sp", "tp"),
        P("tp", "sp"),
    )
    out_specs = P("sp", "tp")
    each = functools.partial(body, mesh.shape["sp"], mesh.shape["tp"])
    return jax.shard_map(each, mesh=mesh, in_specs=in_specs, out_specs=out_specs, check_vma=False)
```

```python
import functools

import jax
import jax.numpy as jnp
from jax import lax
from jax.experimental import pallas as pl
from jax.experimental.pallas import tpu as pltpu
from jax.sharding import PartitionSpec as P

D = 2048
DQK = 128
DV = 256
BLOCK = 64
VALS = 2048


precise = lax.Precision.HIGHEST
norm_eps = 1e-06
very_low = -1e30


def entering(value, axis, join, neutral):
    count, mine = (lax.axis_size(axis), lax.axis_index(axis))
    pieces = jax.tree.map(lambda part: lax.all_gather(part, axis), value)
    subtotal = jax.tree.map(
        lambda part, zero: jnp.full_like(part, 0) + jnp.asarray(zero, part.dtype), value, neutral
    )

    def step(position, subtotal):
        longer = join(subtotal, jax.tree.map(lambda part: part[position], pieces))
        return jax.tree.map(lambda new, old: jnp.where(position < mine, new, old), longer, subtotal)

    return lax.fori_loop(0, count - 1, step, subtotal)


def block_summary(key_blk, value_blk, input_blk, decay_sum):
    decay_total = decay_sum[..., -1]
    log_weight = decay_total[..., None] - decay_sum + input_blk
    weight_peak = jnp.max(log_weight, axis=-1)
    weights = jnp.exp(log_weight - weight_peak[..., None])
    state_mat = jnp.einsum(
        "...ld,...le->...de", weights[..., None] * key_blk, value_blk, precision=precise
    )
    state_vec = jnp.einsum("...l,...ld->...d", weights, key_blk, precision=precise)
    return (state_mat, state_vec, weight_peak, decay_total)


def combine(earlier, later):
    ceiling = jnp.maximum(later[3] + earlier[2], later[2])
    former = jnp.exp(later[3] + earlier[2] - ceiling)
    latter = jnp.exp(later[2] - ceiling)
    return (
        former[..., None, None] * earlier[0] + latter[..., None, None] * later[0],
        former[..., None] * earlier[1] + latter[..., None] * later[1],
        ceiling,
        earlier[3] + later[3],
    )


def block_output(
    query_blk, key_blk, value_blk, input_blk, decay_sum, state_mat, state_vec, state_peak
):
    block_len = query_blk.shape[-2]
    causal = jnp.tril(jnp.ones((block_len, block_len), jnp.bool_))
    log_pair = jnp.where(
        causal,
        decay_sum[..., :, None] - decay_sum[..., None, :] + input_blk[..., None, :],
        -jnp.inf,
    )
    log_carry = decay_sum + state_peak[..., None]
    row_peak = jnp.maximum(log_carry, jnp.max(log_pair, axis=-1))
    scores = jnp.einsum("...ld,...sd->...ls", query_blk, key_blk, precision=precise) * jnp.exp(
        log_pair - row_peak[..., None]
    )
    carried = jnp.exp(log_carry - row_peak)
    numer = jnp.einsum("...ls,...se->...le", scores, value_blk, precision=precise) + carried[
        ..., None
    ] * jnp.einsum("...ld,...de->...le", query_blk, state_mat, precision=precise)
    normer = jnp.sum(scores, axis=-1) + carried * jnp.einsum(
        "...ld,...d->...l", query_blk, state_vec, precision=precise
    )
    denom = jnp.maximum(jnp.abs(normer), jnp.exp(-row_peak))
    return numer / denom[..., None]


def local(
    stream,
    queries,
    keys,
    values,
    out_gate,
    input_gate,
    forget_gate,
    head_gain,
    w_out,
    ffn_gain,
    w_gate,
    w_up,
    w_down,
):
    gate_full, up_full, down_full = (
        lax.all_gather(w_gate, "sp", axis=0, tiled=True),
        lax.all_gather(w_up, "sp", axis=0, tiled=True),
        lax.all_gather(w_down, "sp", axis=1, tiled=True),
    )
    count_of_rows = stream.shape[0]
    head_count = input_gate.shape[1]
    blocks = count_of_rows // BLOCK

    def to_blocks(array, col_width):
        return (
            array.astype(jnp.float32)
            .reshape(blocks, BLOCK, head_count, col_width)
            .transpose(2, 0, 1, 3)
        )

    query_blk = to_blocks(queries, DQK) * DQK ** (-0.5)
    key_blk = to_blocks(keys, DQK)
    value_blk = to_blocks(values, DV)
    input_blk = input_gate.reshape(blocks, BLOCK, head_count).transpose(2, 0, 1)
    decay_sum = jnp.cumsum(
        jax.nn.log_sigmoid(forget_gate).reshape(blocks, BLOCK, head_count).transpose(2, 0, 1),
        axis=-1,
    )
    summary = block_summary(key_blk, value_blk, input_blk, decay_sum)
    identity = (
        jnp.zeros((head_count, DQK, DV), jnp.float32),
        jnp.zeros((head_count, DQK), jnp.float32),
        jnp.full((head_count,), very_low, jnp.float32),
        jnp.zeros((head_count,), jnp.float32),
    )

    def advance(carry, piece):
        return (combine(carry, piece), carry)

    local_total, prefix = lax.scan(
        advance, identity, jax.tree.map(lambda array: jnp.moveaxis(array, 1, 0), summary)
    )
    carry_in = entering(local_total, "sp", combine, identity)
    start = combine(
        jax.tree.map(lambda array: array[:, None], carry_in),
        jax.tree.map(lambda array: jnp.moveaxis(array, 0, 1), prefix),
    )
    mixed_heads = block_output(
        query_blk, key_blk, value_blk, input_blk, decay_sum, start[0], start[1], start[2]
    )
    head_rows = mixed_heads.transpose(1, 2, 0, 3).reshape(count_of_rows, head_count, DV)
    local_sq = jnp.sum(head_rows * head_rows, axis=(1, 2))
    total_sq = lax.psum(local_sq, "tp")
    row_scale = lax.rsqrt(total_sq / VALS + norm_eps)
    gated = (
        head_rows
        * row_scale[:, None, None]
        * head_gain.reshape(head_count, DV)
        * jax.nn.sigmoid(out_gate.astype(jnp.float32).reshape(count_of_rows, head_count, DV))
    )
    heads_out = gated.reshape(count_of_rows, head_count * DV).astype(jnp.bfloat16)
    partial_value = jnp.dot(heads_out, w_out, preferred_element_type=jnp.float32)
    col_width = stream.shape[1]
    col_start = lax.axis_index("tp") * col_width
    mixer_own = lax.psum_scatter(
        partial_value.astype(jnp.bfloat16), "tp", scatter_dimension=1, tiled=True
    ).astype(jnp.float32)
    resid_own = (stream.astype(jnp.float32) + mixer_own).astype(jnp.bfloat16)
    resid_f = resid_own.astype(jnp.float32)
    square_total = lax.psum(jnp.sum(resid_f * resid_f, axis=-1), "tp")
    gain_own = lax.dynamic_slice_in_dim(ffn_gain, col_start, col_width)
    normed_own = (resid_f * lax.rsqrt(square_total / D + norm_eps)[:, None] * gain_own).astype(
        jnp.bfloat16
    )
    normed = lax.all_gather(normed_own, "tp", axis=1, tiled=True)
    gate_act = jnp.dot(normed, gate_full, preferred_element_type=jnp.float32)
    up_act = jnp.dot(normed, up_full, preferred_element_type=jnp.float32)
    hidden = (jax.nn.silu(gate_act) * up_act).astype(jnp.bfloat16)
    term = jnp.dot(hidden, down_full, preferred_element_type=jnp.float32)
    down_own = lax.psum_scatter(
        term.astype(jnp.bfloat16), "tp", scatter_dimension=1, tiled=True
    ).astype(jnp.float32)
    return (resid_own.astype(jnp.float32) + down_own).astype(jnp.bfloat16)


def remote(src, dst, send, recv, target):
    return pltpu.make_async_remote_copy(
        src_ref=src,
        dst_ref=dst,
        send_sem=send,
        recv_sem=recv,
        device_id=target,
        device_id_type=pl.DeviceIdType.MESH,
    )


COPIES = 256
SUMS = 28


def fused_kernel(
    n, m, heads, stream_h, q_h, k_h, v_h, og_h, f_h, i_h, hg_h, wo_h, fg_h, wg_h, wu_h, wd_h,
    out_ref, f_ref, i_ref, hg_ref, fg_ref, kvb, gb, stb, qb, ogb, wob, wgb, wub, wtb, gub, db, pb, pxb, xb, hb, ob, rb, sqb,
    resb, ssem, rsem, lsem, note,
):
    rows, width = out_ref.shape
    ring = n // 2
    half = rows // 2
    dv = width // heads
    dqk = qb.shape[1] // heads
    part, depth = wtb.shape[2], wtb.shape[3]
    room = gub.shape[3]
    low = jnp.bfloat16
    s, t = lax.axis_index("sp"), lax.axis_index("tp")
    z, y, x, c = s // 2, s % 2, t // 2, t % 2
    lead, middle = z % 2 == c, (z == 1) | (z == 2)
    zs = [2 * ((z // 2 + d // 2) % 2) + (z + d) % 2 for d in range(ring)]
    ys, xs, cs = ([y, 1 - y], [x, 1 - x], [c, 1 - c])
    ranks = [[zs[oz] * 2 + ys[oe] for oe in range(2)] for oz in range(ring)]
    cores = [[xs[ox] * 2 + cs[oc] for oc in range(2)] for ox in range(2)]
    places_x = [[xs[ox] * 2 + ty for ty in range(2)] for ox in range(2)]
    places_z = [v // 2 for v in zs]
    at = lambda oz, oe: ranks[oz][oe]
    to = lambda oz=0, oe=0, ox=0, oc=0: (at(oz, oe), cores[ox][oc])
    under = [[(z + ring - d) % ring * 2 + ys[oe] for oe in range(2)] for d in range(ring)]
    above = ((z + 1) % ring * 2 + y, t)
    home = x == z // 2
    branches = {
        "all": None,
        "lead home": lead & home,
        "lead away": lead & jnp.logical_not(home),
        "lead": lead,
        "other": jnp.logical_not(lead),
        "lead0": lead & (c == 0),
        "lead1": lead & (c == 1),
        "lead mid": lead & middle,
        "other one": jnp.logical_not(lead) & (z == 1),
        "other two": jnp.logical_not(lead) & (z == 2),
        "other end": jnp.logical_not(lead | middle),
        "lead end": lead & jnp.logical_not(middle),
        "low y": y == 0,
        "lower": z < 2,
        "upper": z >= 2,
    }
    for d in range(ring):
        branches["at", d] = z == d
        branches["from", d] = z >= d
        branches["up", d] = (z >= d) & (z < ring - 1)

    def when(branch):
        return pl.when(branches[branch])

    first, second = slice(0, half), slice(half, rows)
    places, begun, spots = {}, {}, {}

    def place(key):
        i = places.setdefault(key, len(places))
        assert i < COPIES
        return i

    def begin(branch, key, src, dst, target, tag=""):
        def make():
            return remote(
                src(), dst(), ssem.at[place((key, tag))], rsem.at[place((key, ""))], target
            )

        make().start()
        begun.setdefault(branch, {})[key, tag] = make

    def arrive(key, ref):
        i = place((key, ""))
        remote(ref, ref, ssem.at[i], rsem.at[i], to(0, 0, 0, 1)).wait_recv()

    def spot(key):
        i = spots.setdefault(key, len(spots))
        assert i < SUMS
        return rb.at[i]

    count = [0]

    def local(src, dst):
        copy = pltpu.make_async_copy(src, dst, lsem.at[count[0]])
        count[0] += 1
        copy.start()
        return copy

    qk = heads * dqk
    load_kv = [local(k_h, kvb.at[s, :, :qk]), local(v_h, kvb.at[s, :, qk:])]
    load_w = [local(wg_h, wgb), local(wu_h, wub)]
    load_f = [local(f_h, f_ref), local(i_h, i_ref)]
    load_g = [local(f_h, gb.at[s, 0]), local(i_h, gb.at[s, 1])]
    load_gain = [local(hg_h, hg_ref), local(fg_h, fg_ref)]
    load_cell = [local(q_h, qb), local(og_h, ogb)]
    load_rest = [local(wo_h, wob), local(stream_h, stb.at[c])]

    barrier = pltpu.get_barrier_semaphore()
    peers = [to(oz, oe) for oz in range(ring) for oe in range(2) if oz or oe]
    peers += [to(0, 0, ox, oc) for ox in range(2) for oc in range(2) if ox or oc]
    peers += [to(1, 0, 0, 1), to(2, 0, 0, 1)]
    for peer in peers:
        pl.semaphore_signal(barrier, inc=1, device_id=peer, device_id_type=pl.DeviceIdType.MESH)
    pl.semaphore_wait(barrier, len(peers))

    for copy in load_f:
        copy.wait()
    others = [(oz, oe) for oz in range(ring) for oe in range(2) if oz or oe]
    for oz, oe in others:
        for w, ref in enumerate((f_ref, i_ref)):
            begin(
                "all", ("g", w, oz, oe), lambda ref=ref: ref, lambda w=w: gb.at[s, w],
                to(oz, oe),
            )

    def piece_kv(d, oe, rows_of):
        return kvb.at[under[d][oe]].at[rows_of]

    def kv(branch, d, way, rows_of):
        up = way == "up"
        key = ("kv", d + up, 1 - up, rows_of is second)
        ref = lambda: piece_kv(d, 0, rows_of)
        begin(branch, key, ref, ref, above if up else to(0, 1))

    def kv_in(d, oe, rows_of):
        arrive(("kv", d, oe, rows_of is second), piece_kv(d, oe, rows_of))

    for copy in load_kv:
        copy.wait()

    for rows_of in (first, second):

        @when(("up", 0))
        def _():
            kv(("up", 0), 0, "up", rows_of)

        @when("low y")
        def _():
            kv("low y", 0, "across", rows_of)

    for j in range(1, n - 1):

        @pl.when(j > s)
        def _():
            kvb[j] = jnp.zeros(kvb.shape[1:], low)

    zero = jnp.zeros((room - part, depth), low)
    for k in range(n):
        for core in range(2):
            for w in range(2):
                gub[k, w, core, part:] = zero
                if k < n // 2:
                    db[k, w, core, part:] = zero
    for copy in load_w:
        copy.wait()
    lanes = 128
    for w, source in enumerate((wgb, wub)):
        for q in range(source.shape[1] // lanes):
            turned = source[:, q * lanes : (q + 1) * lanes].T
            cut = q * lanes
            while cut < (q + 1) * lanes:
                stop = min((cut // part + 1) * part, (q + 1) * lanes)
                off = cut % part
                wtb[cut // part, w, off : off + stop - cut] = turned[cut - q * lanes : stop - q * lanes]
                cut = stop

    gu_at = lambda k: gub.at[k, :, c, :part]
    d_at = lambda k: db.at[k, :, c, :part]

    def weights(branch, oz, oe):
        k = at(oz, oe)
        begin(branch, ("gu", oz, oe), lambda: wtb.at[k], lambda: gu_at(s), to(oz, oe))

    quarters = [[zs[oz] % 2 * 2 + ys[oe] for oe in range(2)] for oz in range(2)]
    mine = quarters[0][0]

    def weights_d(oz, oe):
        k = quarters[oz][oe]
        begin("all", ("d", oz, oe), lambda: wd_h.at[:, k], lambda: d_at(mine), to(oz, oe))

    load_own = [local(wtb.at[s], gu_at(s)), local(wd_h.at[:, mine], d_at(mine))]

    near = [(0, 1), (1, 0), (1, 1)]
    far = [(2, 0), (3, 0), (2, 1), (3, 1)]
    plan = {
        0: ([(1, 0), (0, 1)], [], [], [(2, 0), (2, 1), (3, 0), (3, 1), (1, 1)], []),
        1: ([(1, 0)], [(3, 0), (3, 1)], [], [(2, 0), (2, 1), (0, 1), (1, 1)], []),
        2: ([(3, 0), (2, 0)], [], [(1, 0), (3, 1)], [(2, 1), (0, 1)], [(1, 1)]),
        3: ([(2, 0), (3, 0), (1, 0)], [], [(2, 1)], [(3, 1), (0, 1), (1, 1)], []),
    }

    def issue(phase):
        for at_z, phases in plan.items():
            if phases[phase]:

                @when(("at", at_z))
                def _():
                    for oz, oe in phases[phase]:
                        weights(("at", at_z), oz, oe)

    issue(0)

    for d in range(1, ring):
        for rows_of in (first, second):

            @when(("from", d))
            def _():
                kv_in(d, 0, rows_of)
                if d < ring - 1:

                    @when(("up", d))
                    def _():
                        kv(("up", d), d, "up", rows_of)

                kv(("from", d), d, "across", rows_of)

    note_partner = lambda i: pl.semaphore_signal(
        note.at[i], inc=1, device_id=to(0, 0, 0, 1), device_id_type=pl.DeviceIdType.MESH
    )
    note_partner(1)
    pl.semaphore_wait(note.at[1], 1)

    issue(1)

    for rows_of in (first, second):

        @pl.when(y == 1)
        def _():
            kv_in(0, 1, rows_of)

        for d in range(1, ring):

            @when(("from", d))
            def _():
                kv_in(d, 1, rows_of)

    issue(2)
    for oz, oe in others:
        for w in range(2):
            arrive(("g", w, oz, oe), gb.at[at(oz, oe), w])
    for copy in load_cell + load_g + load_gain + load_rest:
        copy.wait()

    @when("other")
    def _():
        begin("other", ("st",), lambda: stb.at[c], lambda: stb.at[c], to(0, 0, 0, 1))

    at_row = lax.broadcasted_iota(jnp.int32, (rows, rows), 0)
    at_col = lax.broadcasted_iota(jnp.int32, (rows, rows), 1)
    eye, causal = at_row == at_col, at_row >= at_col
    to_column = lambda row: jnp.sum(jnp.where(eye, row, 0.0), axis=1, keepdims=True)
    upper = (at_row <= at_col).astype(jnp.float32)
    gates = jnp.concatenate([gb[j, 0] for j in range(n)], axis=0)
    entries = jnp.concatenate([gb[j, 1] for j in range(n)], axis=0)
    log_sigmoid = lambda v: jnp.minimum(v, 0.0) - jnp.log1p(jnp.exp(-jnp.abs(v)))
    decays = jnp.dot(
        log_sigmoid(gates), upper, precision=precise, preferred_element_type=jnp.float32
    )
    own_decay = jnp.dot(
        log_sigmoid(f_ref[...]), upper, precision=precise, preferred_element_type=jnp.float32
    )
    own_entry = i_ref[...]
    square = jnp.zeros((rows, 1), jnp.float32)
    gated = []
    for h in range(heads):
        decay_row = own_decay[h : h + 1]
        decay_col = to_column(decay_row)
        after = jnp.zeros((1, 1), jnp.float32)
        peak = jnp.full((1, 1), very_low, jnp.float32)
        weigh = [None] * n
        for j in reversed(range(n)):
            earlier = j < s
            block = decays[j * heads + h : j * heads + h + 1]
            total = block[:, rows - 1 :]
            entry = entries[j * heads + h : j * heads + h + 1]
            weigh[j] = jnp.where(earlier, total - block + entry + after, very_low)
            after = after + jnp.where(earlier, total, 0.0)
            peak = jnp.maximum(peak, jnp.max(weigh[j], axis=1, keepdims=True))
        pair = jnp.where(causal, decay_col - decay_row + own_entry[h : h + 1], very_low)
        row_peak = jnp.maximum(decay_col + peak, jnp.max(pair, axis=1, keepdims=True))
        query = qb[:, h * dqk : (h + 1) * dqk]
        numer = jnp.zeros((rows, dv), jnp.float32)
        normer = jnp.zeros((rows, 1), jnp.float32)

        def add(numer, normer, j, log_weight):
            key = kvb[j, :, h * dqk : (h + 1) * dqk]
            value = kvb[j, :, qk + h * dv : qk + (h + 1) * dv]
            scores = lax.dot_general(
                query, key, (((1,), (1,)), ((), ())), preferred_element_type=jnp.float32
            )
            scores = scores * dqk ** (-0.5) * jnp.exp(log_weight - row_peak)
            high = scores.astype(low)
            rest = (scores - high.astype(jnp.float32)).astype(low)
            numer = (
                numer
                + jnp.dot(high, value, preferred_element_type=jnp.float32)
                + jnp.dot(rest, value, preferred_element_type=jnp.float32)
            )
            return numer, normer + jnp.sum(scores, axis=1, keepdims=True)

        numer, normer = add(numer, normer, s, pair)
        for j in range(n - 1):
            numer, normer = add(numer, normer, j, decay_col + weigh[j])
        cell = numer / jnp.maximum(jnp.abs(normer), jnp.exp(-row_peak))
        square = square + jnp.sum(cell * cell, axis=1, keepdims=True)
        span = slice(h * dv, (h + 1) * dv)
        gate = 1.0 / (1.0 + jnp.exp(-ogb[:, span].astype(jnp.float32)))
        gated.append((cell * hg_ref[:, span] * gate).astype(low))
    heads_out = jnp.concatenate(gated, axis=1)
    square_row = jnp.sum(jnp.where(eye, square, 0.0), axis=0, keepdims=True)
    sqb[t] = jnp.broadcast_to(square_row, sqb.shape[1:])
    for ox in range(2):
        for oc in range(2):
            if ox or oc:
                square_at = lambda: sqb.at[t]
                begin("all", ("sq", ox, oc), square_at, square_at, to(0, 0, ox, oc))

    def mixer_part(ox, oc):
        j = xs[ox] * 2 + oc
        cols = pl.ds(pl.multiple_of(j * width, width), width)
        pb[2 * ox + oc] = jnp.dot(
            heads_out, wob[:, cols], preferred_element_type=jnp.float32
        ).astype(low)

    def plus(ref, other):
        ref[...] = (ref[...].astype(jnp.float32) + other[...].astype(jnp.float32)).astype(low)

    x_at = lambda oz, oe, ox, ty: xb.at[places_z[oz], ys[oe], places_x[ox][ty]]

    @when("other")
    def _():
        for ox in (1, 0):
            for oc in range(2):
                mixer_part(ox, oc)
                begin(
                    "other", ("pc", ox, oc), lambda i=2 * ox + oc: pb.at[i],
                    lambda i=2 * ox + oc: spot(("pc", i)), to(0, 0, 0, 1),
                )

    hops = {"out": (1, 0, 0), "in": (3, 0, 0), "y": (0, 1, 0), "x": (0, 0, 1)}

    def forward(branch, oz, oe, ox, ty, way):
        tz, te, tx = hops[way]
        key = ("x", ty, oz ^ tz, oe ^ te, ox ^ tx)
        ref = lambda: x_at(oz, oe, ox, ty)
        begin(branch, key, ref, ref, to(tz, te, tx), way)

    def spread(branch, oz, ty, ways):
        for way in ways:
            forward(branch, oz, 0, 0, ty, way)
        for turn in ("y", "x"):
            forward(branch, oz, 0, 0, ty, turn)

    def x_in(oz, oe, ox, ty):
        arrive(("x", ty, oz, oe, ox), x_at(oz, oe, ox, ty))

    @pl.when(lead)
    def _():
        for oc in range(2):
            mixer_part(1, oc)
            arrive(("pc", 1, oc), spot(("pc", 2 + oc)))
            plus(pb.at[2 + oc], spot(("pc", 2 + oc)))
            begin(
                "lead", ("px", oc), lambda i=2 + oc: pb.at[i], lambda oc=oc: pxb.at[oc],
                to(0, 0, 1),
            )
        for oc in range(2):
            mixer_part(0, oc)
            arrive(("pc", 0, oc), spot(("pc", oc)))
            plus(pb.at[oc], spot(("pc", oc)))
        arrive(("st",), stb.at[1 - c])

    for ox in range(2):
        for oc in range(2):
            if ox or oc:
                arrive(("sq", ox, oc), sqb.at[xs[ox] * 2 + cs[oc]])

    @pl.when(lead)
    def _():
        total_sq = to_column(jnp.sum(sqb[...], axis=0)[0:1])
        row_scale = lax.rsqrt(total_sq / (m * width) + norm_eps)
        for oc in (1, 0):
            arrive(("px", oc), pxb.at[oc])
            mixer = (pb[oc].astype(jnp.float32) + pxb[oc].astype(jnp.float32)) * row_scale
            own = x_at(0, 0, 0, oc)
            own[...] = (stb[oc].astype(jnp.float32) + mixer).astype(low)


            for branch, ways in (("lead mid", ("in", "out")), ("lead end", ("out",))):

                @when(branch)
                def _():
                    spread(branch, 0, oc, ways)


        begin(
            "lead", ("res",), lambda: xb.at[places_z[0], y, cores[0][1]], lambda: resb, to(0, 0, 0, 1)
        )
        resb[...] = xb[places_z[0], y, cores[0][0]]

    def pass_on(branch, oz, *ways):
        for ty in (1, 0):
            x_in(oz, 0, 0, ty)
            spread(branch, oz, ty, ways)

    @when("other end")
    def _():
        pass_on("other end", 1)

    @when("other two")
    def _():
        pass_on("other two", 3, "out")
        pass_on("other two", 1, "in")

    @when("other one")
    def _():
        pass_on("other one", 1, "in")
        for ty in (1, 0):
            begun["other one"].pop((("x", ty, 2, 0, 0), "in"))().wait_send()
        for oc in range(2):
            pl.semaphore_signal(
                note.at[0], inc=1, device_id=to(1, 0, 0, oc), device_id_type=pl.DeviceIdType.MESH
            )

    @when(("at", 0))
    def _():
        pl.semaphore_wait(note.at[0], 1)

    issue(3)


    for copy in load_own:
        copy.wait()

    def share(oz, oe):
        k = at(oz, oe)
        if oz or oe:
            arrive(("gu", oz, oe), gu_at(k))
        begin("all", ("gus", oz, oe), lambda: gu_at(k), lambda: gu_at(k), to(0, 0, 0, 1))

    def share_d(oz, oe):
        k = quarters[oz][oe]
        if oz or oe:
            arrive(("d", oz, oe), d_at(k))
        begin("all", ("ds", oz, oe), lambda: d_at(k), lambda: d_at(k), to(0, 0, 0, 1))

    @when("lead mid")
    def _():
        pass_on("lead mid", 2, "out")

    @when("lead end")
    def _():
        pass_on("lead end", 2)

    @when("other one")
    def _():
        pass_on("other one", 3, "out")

    @when("other end")
    def _():
        pass_on("other end", 3)

    issue(4)
    sides = {"lead": (0, 2), "other": (1, 3)}
    for role, zones in sides.items():

        @when(role)
        def _():
            for oz in zones:
                for ty in (1, 0):
                    x_in(oz, 1, 0, ty)
                    forward(role, oz, 1, 0, ty, "x")

    for oz, oe in near:
        weights_d(oz, oe)
    share(0, 0)
    for oz, oe in near:
        share(oz, oe)

    for oz, oe in far[:2]:
        share(oz, oe)

    for oz, oe in far[2:]:
        share(oz, oe)

    for role, zones in sides.items():

        @when(role)
        def _():
            for oz in zones:
                for oe in range(2):
                    for ty in (1, 0):
                        x_in(oz, oe, 1, ty)

    for oz, oe in [(0, 0)] + near + far:
        arrive(("gus", oz, oe), gub.at[at(oz, oe), :, 1 - c, :part])

    nt = (((1,), (1,)), ((), ()))
    per = width // depth
    wide = 2 * room

    zone = z // 2

    def gate(i):
        size = 2 * rows
        squares = jnp.zeros((size, 1), jnp.float32)
        for j in range(m):
            piece = xb[i, :, j].reshape(size, width).astype(jnp.float32)
            squares = squares + jnp.sum(piece * piece, axis=1, keepdims=True)
        scale = lax.rsqrt(squares / (m * width) + norm_eps)
        act = jnp.zeros((size, 2 * wide), jnp.float32)
        for k in range(n):
            j, a = k // per, (k % per) * depth
            piece = xb[i, :, j, :, a : a + depth].reshape(size, depth).astype(jnp.float32)
            normed = (piece * scale * fg_ref[:, k * depth : (k + 1) * depth]).astype(low)
            act += lax.dot_general(
                normed, gub[k].reshape(2 * wide, depth), nt, preferred_element_type=jnp.float32
            )
        gate_act, up_act = act[:, :wide], act[:, wide:]
        hb[i, zone] = (gate_act / (1.0 + jnp.exp(-gate_act)) * up_act).astype(low)
        ref = lambda: hb.at[i, zone]
        begin("all", ("hid", i), ref, ref, to(2))

    def down(i):
        arrive(("hid", i), hb.at[i, 1 - zone])
        for k in range(n // 2):
            total = jnp.zeros((2 * rows, depth), jnp.float32)
            for w in range(2):
                total += jnp.dot(
                    hb[i, w], db[k, w].reshape(wide, depth), preferred_element_type=jnp.float32
                )
            j, a = k // per, (k % per) * depth
            ob[i, :, j, :, a : a + depth] = total.astype(low).reshape(2, rows, depth)

    gate(0)
    gate(1)
    share_d(0, 0)
    for oz, oe in near:
        share_d(oz, oe)
    for oz, oe in [(0, 0)] + near:
        arrive(("ds", oz, oe), db.at[quarters[oz][oe], :, 1 - c, :part])

    o_at = lambda oz, oe, ty: ob.at[places_z[oz], ys[oe], ty]

    def give(branch, stage, oz, oe, ty, way):
        tz, te, tx = hops[way]
        key = (stage, oz ^ tz, oe ^ te, ty)
        place = (stage, (oz ^ tz) // 2, oe ^ te, ty)
        begin(branch, key, lambda: o_at(oz, oe, ty), lambda: spot(place), to(tz, te, tx))

    def take(stage, oz, oe, ty):
        key, got = (stage, oz, oe, ty), spot((stage, oz // 2, oe, ty))
        arrive(key, got)
        plus(o_at(oz, oe, ty), got)

    def start(branch, oz):
        give(branch, "ry", oz, 1, 0, "y")
        if branch == "other":
            for oe in (1, 0):
                give(branch, "rz", oz, oe, 1, "out")

    for i in range(2):
        down(i)

        @when("lead")
        def _():
            for oz in (0, 2):

                @pl.when(places_z[oz] == i)
                def _():
                    start("lead", oz)

        @when("other")
        def _():
            for oz in (1, 3):

                @pl.when(places_z[oz] == i)
                def _():
                    start("other", oz)

    @when("other")
    def _():
        for oz in (3, 1):
            take("ry", oz, 0, 0)
            give("other", "rz", oz, 0, 0, "out")

    @when("lead")
    def _():
        for oz in (2, 0):
            take("rz", oz, 1, 1)
            give("lead", "ry", oz, 1, 1, "y")
            take("ry", oz, 0, 0)
            take("rz", oz, 0, 1)
        for oz in (2, 0):
            for ty in range(2):
                take("rz" if ty == 0 else "ry", oz, 0, ty)

                @when("lead away")
                def _():
                    give("lead away", "rx", oz, 0, ty, "x")

                @when("lead home")
                def _():
                    take("rx", oz, 0, ty)
                    if oz:
                        target = (at(2, 0), places_x[0][ty])
                        begin(
                            "lead home", ("rf", ty), lambda ty=ty: o_at(2, 0, ty),
                            lambda: spot(("rf",)), target,
                        )

        @when("lead home")
        def _():
            begin(
                "lead home", ("base",), lambda: ob.at[places_z[0], y, 1 - c],
                lambda: spot(("rf",)), to(0, 0, 0, 1),
            )
            spot(("rf",))[...] = ob[places_z[0], y, c]

    @when("other")
    def _():
        arrive(("res",), resb)

        @pl.when(home)
        def _():
            arrive(("base",), spot(("rf",)))

    @pl.when(jnp.logical_not(home))
    def _():
        for ty in range(2):

            @pl.when(c == ty)
            def _():
                arrive(("rf", ty), spot(("rf",)))

    total = resb[...].astype(jnp.float32) + spot(("rf",))[...].astype(jnp.float32)
    out_ref[...] = total.astype(low)

    for branch, condition in branches.items():

        def finish(branch=branch):
            for make in begun.get(branch, {}).values():
                make().wait_send()

        if condition is None:
            finish()
        else:
            pl.when(condition)(finish)


def fused(
    n, m, stream, queries, keys, values, out_gate, input_gate, forget_gate, head_gain, w_out,
    ffn_gain, w_gate, w_up, w_down,
):
    rows, width = stream.shape
    heads = input_gate.shape[1]
    depth, hidden = w_gate.shape
    part = hidden // n
    room = -(-part // 64) * 64
    low = jnp.bfloat16
    dma = pltpu.SemaphoreType.DMA
    vmem = pl.BlockSpec(memory_space=pltpu.VMEM)
    hbm = pl.BlockSpec(memory_space=pltpu.HBM)
    buffer = lambda *shape: pltpu.VMEM(shape, low)
    piece = (rows, width)
    return pl.pallas_call(
        functools.partial(fused_kernel, n, m, heads),
        out_shape=jax.ShapeDtypeStruct(piece, low),
        in_specs=[hbm] * 13,
        out_specs=vmem,
        scratch_shapes=[
            pltpu.VMEM((heads, rows), jnp.float32),
            pltpu.VMEM((heads, rows), jnp.float32),
            pltpu.VMEM((1, head_gain.shape[0]), jnp.float32),
            pltpu.VMEM((1, ffn_gain.shape[0]), jnp.float32),
            buffer(n, rows, keys.shape[1] + values.shape[1]),
            pltpu.VMEM((n, 2, heads, rows), jnp.float32),
            buffer(2, *piece),
            buffer(*queries.shape),
            buffer(*out_gate.shape),
            buffer(*w_out.shape),
            buffer(*w_gate.shape),
            buffer(*w_up.shape),
            buffer(n, 2, part, depth),
            buffer(n, 2, 2, room, depth),
            buffer(n // 2, 2, 2, room, depth),
            buffer(m, *piece),
            buffer(2, *piece),
            buffer(n // 4, 2, m, *piece),
            buffer(2, 2, 2 * rows, 2 * room),
            buffer(n // 4, 2, 2, *piece),
            buffer(SUMS, *piece),
            pltpu.VMEM((m, 8, rows), jnp.float32),
            buffer(*piece),
            dma((COPIES,)),
            dma((COPIES,)),
            dma((20,)),
            pltpu.SemaphoreType.REGULAR((2,)),
        ],
        compiler_params=pltpu.CompilerParams(
            collective_id=0, has_side_effects=True, vmem_limit_bytes=60 * 2**20
        ),
    )(
        stream, queries, keys, values, out_gate, forget_gate.T, input_gate.T,
        head_gain.reshape(1, -1), w_out, ffn_gain.reshape(1, -1), w_gate, w_up,
        w_down.reshape(2, n // 2, part, depth),
    )


def fits(n, m, stream, input_gate, w_gate):
    rows, width = stream.shape
    depth, hidden = w_gate.shape
    shaped = n // 2 == 4 and n % 2 == 0 and m == 4
    tiled = hidden % (16 * n) == 0 and hidden % 128 == 0 and depth % 128 == 0
    even = width % depth == 0 and rows == 128 and m * width == n * depth
    held = rows * width * 2 * 80 + 24 * depth * hidden
    return shaped and tiled and even and input_gate.shape[1] <= 4 and held < 40 * 2**20


def body(n, m, *arrays):
    if fits(n, m, arrays[0], arrays[5], arrays[10]):
        return fused(n, m, *arrays)
    return local(*arrays)


def solution(mesh):
    in_specs = (
        P("sp", "tp"),
        P("sp", "tp"),
        P("sp", "tp"),
        P("sp", "tp"),
        P("sp", "tp"),
        P("sp", "tp"),
        P("sp", "tp"),
        P("tp"),
        P("tp", None),
        P(),
        P("sp", "tp"),
        P("sp", "tp"),
        P("tp", "sp"),
    )
    out_specs = P("sp", "tp")
    each = functools.partial(body, mesh.shape["sp"], mesh.shape["tp"])
    return jax.shard_map(each, mesh=mesh, in_specs=in_specs, out_specs=out_specs, check_vma=False)
```
